256 devices in a mesh: sp: 32 (over z, x), tp: 8 (over y, core).
Axes of the slice: x: 4, y: 4, z: 8, core: 2. Of those that a mesh axis runs over, the one named last changes fastest.
Arguments:
- prompt_tokens: bfloat16 [65536, 2048], P(('sp', 'tp')), may hold values from -8 to 8
- key_weight: bfloat16 [2048, 2048], P(None, 'tp'), may hold values from -0.125 to 0.125
- value_weight: bfloat16 [2048, 4096], P(None, 'tp'), may hold values from -0.125 to 0.125
- input_weight: bfloat16 [2048, 32], replicated, may hold values from -4 to 4
- forget_weight: bfloat16 [2048, 32], replicated, may hold values from -0.125 to 0.125
- forget_bias: float32 [32], replicated, as said below
- new_token: bfloat16 [2048], replicated, may hold values from -8 to 8
- new_query: bfloat16 [2048], P('tp'), may hold values from -6 to 6
Outputs:
- key_cache: bfloat16 [65536, 2048], P('sp', 'tp')
- value_cache: bfloat16 [65536, 4096], P('sp', 'tp')
- cache_weight: float32 [32, 65536], P('tp', 'sp')
- reading: float32 [4096], P('tp')
The draws below stay inside these ranges and needn't reach their ends.
Inputs may be any that keep to these rules, and one draw needn't show every extreme that they name: `forget_bias`: every head's forget gate offset is 2 or more.
All inputs are finite; a program needn't handle non-finite values.
Results may differ from the reference program's by a relative error of at most 0.0058.
Values may be sent and summed in bfloat16 or wider, within the bound.
A program may use at most 64 MiB of HBM per device.

```python
import math
import jax
import jax.numpy as jnp
from jax import lax

D = 2048
H = 32
DQK = 64
DV = 128
LEN = 65536


def draw_prompt_tokens(key, part):
    base_key = jax.random.fold_in(key, 11)
    scale_key = jax.random.fold_in(key, 12)
    base_draw = jnp.clip(jax.random.normal(base_key, (LEN, D), jnp.float32), -5.0, 5.0)
    block_count = LEN // 32
    block_scales = jnp.exp(jax.random.uniform(scale_key, (block_count, 1), jnp.float32, math.log(0.5), math.log(1.6)))
    block_scales = jnp.repeat(block_scales, 32, axis=0)
    return (base_draw * block_scales).astype(jnp.bfloat16)


def draw_input_weight(key, part):
    base_draw = jnp.clip(jax.random.normal(jax.random.fold_in(key, 21), (D, H), jnp.float32), -4.0, 4.0) * D ** (-0.5)
    return base_draw.astype(jnp.bfloat16)


def draw_forget_bias(key, part):
    picked = jax.random.uniform(jax.random.fold_in(key, 31), (H,), jnp.float32)
    quick_rates = jax.random.uniform(jax.random.fold_in(key, 32), (H,), jnp.float32, 3.0, 4.5)
    slow_rates = math.log(LEN) + jax.random.uniform(jax.random.fold_in(key, 33), (H,), jnp.float32, 0.0, 1.5)
    quick_share = 0.5
    return jnp.where(picked < quick_share, quick_rates, slow_rates)


def level_of(key, dims, split, low, largest):
    factor_of, own = 1.0, jax.random.fold_in(key, 6)
    for axis_at, shards_of in split:
        steps = jnp.exp(jax.random.uniform(jax.random.fold_in(own, axis_at), (shards_of,), jnp.float32, low / len(split), largest / len(split)))
        factor_of = factor_of * jnp.repeat(steps, dims[axis_at] // shards_of).reshape([-1 if axis == axis_at else 1 for axis in range(len(dims))])
    return factor_of


def centred(own_key, extent, spread, limit, pieces=(), kind=jnp.bfloat16):
    factor_of = level_of(own_key, extent, pieces, -0.22, 0.18) if pieces else 1.0
    drawn = jax.random.normal(own_key, extent, jnp.float32) * spread * factor_of
    return jnp.minimum(jnp.maximum(drawn, -limit), limit).astype(kind)


def setup_inputs(seed: int = 0) -> dict:
    streams_of = jax.random.split(jax.random.key(seed), 9)
    prompt_tokens = draw_prompt_tokens(jax.random.fold_in(streams_of[8], 71), 0)
    key_weight = centred(streams_of[1], (D, H * DQK), D ** -0.5, 0.125, ((1, 8),))
    value_weight = centred(streams_of[2], (D, H * DV), D ** -0.5, 0.125, ((1, 8),))
    input_weight = draw_input_weight(jax.random.fold_in(streams_of[8], 71), 0)
    forget_weight = centred(streams_of[4], (D, H), D ** -0.5, 0.125)
    forget_bias = draw_forget_bias(jax.random.fold_in(streams_of[8], 71), 0)
    new_token = centred(streams_of[6], (D,), 2.0, 8.0)
    new_query = centred(streams_of[7], (H * DQK,), 1.0, 6.0, ((0, 8),))
    return {"prompt_tokens": prompt_tokens, "key_weight": key_weight, "value_weight": value_weight, "input_weight": input_weight, "forget_weight": forget_weight, "forget_bias": forget_bias, "new_token": new_token, "new_query": new_query}


def reference(prompt_tokens, key_weight, value_weight, input_weight, forget_weight, forget_bias, new_token, new_query):
    key_cache = jnp.dot(prompt_tokens, key_weight, preferred_element_type=jnp.float32).astype(jnp.bfloat16)
    value_cache = jnp.dot(prompt_tokens, value_weight, preferred_element_type=jnp.float32).astype(jnp.bfloat16)
    input_gate = jnp.dot(prompt_tokens, input_weight, preferred_element_type=jnp.float32)
    log_forget = jax.nn.log_sigmoid(jnp.dot(prompt_tokens, forget_weight, preferred_element_type=jnp.float32) + forget_bias)
    log_weight = input_gate + (lax.optimization_barrier(jnp.sum(log_forget, axis=0, keepdims=True)) - jnp.cumsum(log_forget, axis=0))
    peak_log = lax.optimization_barrier(jnp.max(log_weight, axis=0))
    cache_weight = jnp.transpose(jnp.exp(log_weight - peak_log[None, :]), (1, 0))
    new_key = jnp.dot(new_token, key_weight, preferred_element_type=jnp.float32).astype(jnp.bfloat16)
    new_value = jnp.dot(new_token, value_weight, preferred_element_type=jnp.float32).astype(jnp.bfloat16)
    new_gate = jnp.dot(new_token, input_weight, preferred_element_type=jnp.float32)
    new_forget = jax.nn.log_sigmoid(jnp.dot(new_token, forget_weight, preferred_element_type=jnp.float32) + forget_bias)
    stable_level = jnp.maximum(new_forget + peak_log, new_gate)
    query_heads = new_query.astype(jnp.float32).reshape(H, DQK)
    key_heads = key_cache.astype(jnp.float32).reshape(LEN, H, DQK)
    key_score = jnp.einsum('shd,hd->sh', key_heads, query_heads, precision=lax.Precision.HIGHEST) / math.sqrt(DQK)
    new_heads = new_key.astype(jnp.float32).reshape(H, DQK)
    new_score = jnp.einsum('hd,hd->h', new_heads, query_heads, precision=lax.Precision.HIGHEST) / math.sqrt(DQK)
    weighted = jnp.exp(new_forget[None, :] + log_weight - stable_level[None, :]) * key_score
    weighted_low = weighted.astype(jnp.bfloat16)
    own_term = jnp.exp(new_gate - stable_level) * new_score
    value_heads = value_cache.astype(jnp.float32).reshape(LEN, H, DV)
    numerator = jnp.einsum('sh,she->he', weighted_low.astype(jnp.float32), value_heads, precision=lax.Precision.HIGHEST)
    numerator = numerator + own_term[:, None] * new_value.astype(jnp.float32).reshape(H, DV)
    denominator = lax.optimization_barrier(jnp.sum(weighted, axis=0)) + own_term
    reading = numerator / jnp.maximum(jnp.abs(denominator), 1.0)[:, None]
    return (key_cache, value_cache, cache_weight, reading.reshape(H * DV))
```

```python
import functools
import math

import jax
import jax.numpy as jnp
from jax import lax
from jax.experimental import pallas as pl
from jax.experimental.pallas import tpu as pltpu
from jax.sharding import Mesh
from jax.sharding import PartitionSpec as P

DQK = 64
DV = 128
SP = ("sp_0", "sp_1")
SP_TP = ("sp_0", "sp_1", "tp")
MESH = pl.DeviceIdType.MESH
F32 = jnp.float32
BF16 = jnp.bfloat16
CHUNK = 32
EARLY = 3


def log_sigmoid(v):
    u = jnp.exp(-jnp.abs(v))
    w = 1.0 + u
    grown = w - 1.0
    tail = jnp.where(grown == 0.0, u, jnp.log(w) * (u / jnp.where(grown == 0.0, 1.0, grown)))
    return -(jnp.maximum(-v, 0.0) + tail)


def remote(src, dst, send, recv, where):
    return pltpu.make_async_remote_copy(
        src_ref=src, dst_ref=dst, send_sem=send, recv_sem=recv, device_id=where, device_id_type=MESH
    )


def kernel(
    tok, kw, vw, iw, fw, fb, nt, nq,
    kout, vout, cwout, rdout,
    xown, xsib, gat, wk, wv, wi, wf,
    sendb, recvb, ngate, nforget, wlog, cpay, cxs, crow, czs, dpay, dxs, drow, dzs, acc, den,
    lsem, own_s, own_r, fwd_s, sib_s, sib_r, osib_s, osib_r,
    b_s, b_r, cx_s, cx_r, cz_s, cz_r, dx_s, dx_r, dz_s, dz_r,
):
    nz, nx, ntp = (lax.axis_size(a) for a in ("sp_0", "sp_1", "tp"))
    z, x, t = (lax.axis_index(a) for a in ("sp_0", "sp_1", "tp"))
    flip = 1 - 2 * (t % 2)
    sib = t + flip
    up, dn = (t + 2) % ntp, (t + ntp - 2) % ntp
    rows = xown.shape[0]
    nchunk = rows // CHUNK

    loads = [
        pltpu.make_async_copy(src, dst, lsem.at[i])
        for i, (src, dst) in enumerate(
            ((tok, xown), (iw, wi), (fw, wf), (kw, wk), (vw, wv))
        )
    ]
    for load in loads:
        load.start()

    barrier = pltpu.get_barrier_semaphore()
    for axis, here, size in (("tp", t, ntp), ("sp_1", x, nx), ("sp_0", z, nz)):
        for d in range(1, size):
            pl.semaphore_signal(
                barrier, inc=1, device_id={axis: (here + d) % size}, device_id_type=MESH
            )
    pl.semaphore_wait(barrier, ntp + nx + nz - 3)

    def own_copies(c):
        piece = xown.at[pl.ds(c * CHUNK, CHUNK)]
        return (
            remote(piece, gat.at[c, pl.ds(0, CHUNK)], own_s.at[0, c], own_r.at[0, c], {"tp": up}),
            remote(
                piece, gat.at[c, pl.ds(CHUNK, CHUNK)], own_s.at[1, c], own_r.at[1, c], {"tp": dn}
            ),
        )

    def send_own(c, carry):
        for copy in own_copies(c):
            copy.start()
        return carry

    def to_sibling(g):
        return remote(
            gat.at[g, pl.ds(0, 2 * CHUNK)],
            gat.at[g, pl.ds(2 * CHUNK, 2 * CHUNK)],
            sib_s.at[g],
            sib_r.at[g],
            {"tp": sib},
        )

    loads[0].wait()
    lax.fori_loop(0, EARLY, send_own, 0)
    own_to_sib = remote(xown, xsib, osib_s, osib_r, {"tp": sib})
    own_to_sib.start()

    loads[1].wait()
    loads[2].wait()
    bias = fb[...]
    token16 = jnp.broadcast_to(nt[...], (16, nt.shape[1]))
    xin = xown[...]
    gate = jnp.dot(xin, wi[...], preferred_element_type=F32)
    forget = log_sigmoid(jnp.dot(xin, wf[...], preferred_element_type=F32) + bias)
    gate_t = gate.T
    forget_t = forget.T
    heads = gate_t.shape[0]
    hd = heads // ntp
    later_mask = (
        lax.broadcasted_iota(jnp.int32, (rows, rows), 0)
        > lax.broadcasted_iota(jnp.int32, (rows, rows), 1)
    ).astype(F32).astype(BF16)
    high = forget_t.astype(BF16)
    rest = forget_t - high.astype(F32)
    mid = rest.astype(BF16)
    low = (rest - mid.astype(F32)).astype(BF16)
    suffix = (
        jnp.dot(low, later_mask, preferred_element_type=F32)
        + jnp.dot(mid, later_mask, preferred_element_type=F32)
        + jnp.dot(high, later_mask, preferred_element_type=F32)
    )
    logw = gate_t + suffix
    total = jnp.broadcast_to(suffix[:, 0:1] + forget_t[:, 0:1], (heads, rows))
    new_g = jnp.dot(token16, wi[...], preferred_element_type=F32)
    new_f = log_sigmoid(jnp.dot(token16, wf[...], preferred_element_type=F32) + bias)
    new_gt = jnp.broadcast_to(new_g.T[:, 0:1], (heads, 128))
    new_ft = jnp.broadcast_to(new_f.T[:, 0:1], (heads, 128))
    for j in range(ntp):
        pick = slice(j * hd, (j + 1) * hd)
        sendb[j, 0:hd, :] = logw[pick]
        sendb[j, hd : 2 * hd, :] = total[pick]
        ngate[j, 0:hd, :] = new_gt[pick]
        ngate[j, hd : 2 * hd, :] = new_gt[pick]
        nforget[j, 0:hd, :] = new_ft[pick]
        nforget[j, hd : 2 * hd, :] = new_ft[pick]

    def across(src, dst_slots, here, size, axis, send, recv):
        copies = []
        for d in range(1, size):
            to = (here + d) % size
            copies.append(
                remote(src(to), dst_slots.at[here], send.at[d - 1], recv.at[d - 1], {axis: to})
            )
        for copy in copies:
            copy.start()
        return copies

    b_copies = across(lambda to: sendb.at[to], recvb, t, ntp, "tp", b_s, b_r)
    recvb[t] = sendb[t]
    lax.fori_loop(EARLY, nchunk, send_own, 0)

    def project(lhs):
        k = jnp.dot(lhs, wk[...], preferred_element_type=F32).astype(BF16)
        v = jnp.dot(lhs, wv[...], preferred_element_type=F32).astype(BF16)
        return k, v

    loads[3].wait()
    loads[4].wait()
    new_k, new_v = project(token16)

    def whole_block(src, source):
        k, v = project(src[...])
        at = pl.ds(pl.multiple_of(source * rows, rows), rows)
        kout[at, :] = k
        vout[at, :] = v

    whole_block(xown, t)

    for copy in b_copies:
        copy.wait_recv()
    zero = jnp.zeros((hd, 128), F32)
    later = zero
    best = None
    for s in reversed(range(ntp)):
        tile = recvb[s]
        for half in (1, 0):
            part = tile[0:hd, half * 128 : (half + 1) * 128] + later
            wlog[2 * s + half, 0:hd, :] = part
            wlog[2 * s + half, hd : 2 * hd, :] = zero
            best = part if best is None else jnp.maximum(best, part)
        later = later + tile[hd : 2 * hd, 0:128]
    block_peak = jnp.broadcast_to(jnp.max(best, axis=1, keepdims=True), (hd, 128))
    cpay[0:hd, :] = later
    cpay[hd : 2 * hd, :] = block_peak
    cx_copies = across(lambda to: cpay, cxs, x, nx, "sp_1", cx_s, cx_r)
    cxs[x] = cpay[...]

    own_to_sib.wait_recv()
    whole_block(xsib, sib)

    for copy in cx_copies:
        copy.wait_recv()

    def scanned(slots, size, here):
        behind = zero
        mine = zero
        peak = None
        for s in reversed(range(size)):
            tile = slots[s]
            candidate = tile[hd : 2 * hd] + behind
            peak = candidate if peak is None else jnp.maximum(peak, candidate)
            mine = mine + jnp.where(s > here, tile[0:hd], zero)
            behind = behind + tile[0:hd]
        return behind, peak, mine

    row_total, row_peak, later_x = scanned(cxs, nx, x)
    crow[0:hd, :] = row_total
    crow[hd : 2 * hd, :] = row_peak
    cz_copies = across(lambda to: crow, czs, z, nz, "sp_0", cz_s, cz_r)
    czs[z] = crow[...]

    def ship(g):
        pltpu.make_async_copy(gat.at[g, pl.ds(0, CHUNK)], gat.at[g, pl.ds(0, CHUNK)], own_r.at[0, g]).wait()
        pltpu.make_async_copy(gat.at[g, pl.ds(0, CHUNK)], gat.at[g, pl.ds(0, CHUNK)], own_r.at[1, g]).wait()
        to_sibling(g).start()

    def forward(g, side):
        half = pl.ds(side * CHUNK, CHUNK)
        return remote(
            gat.at[g, half],
            gat.at[nchunk + g // 2, half],
            fwd_s.at[g],
            own_r.at[side, nchunk + g // 2],
            {"tp": dn if side else up},
        )

    def arrive(g):
        pltpu.make_async_copy(
            gat.at[g, pl.ds(0, 2 * CHUNK)], gat.at[g, pl.ds(0, 2 * CHUNK)], sib_r.at[g]
        ).wait()
        k, v = project(gat[g])
        e = g // nchunk
        c0 = g + e * (g - 2 * nchunk)
        s0 = (t + ntp - 2 - 2 * e) % ntp
        s1 = (t + 2 + 2 * e) % ntp
        starts = (
            s0 * rows + c0 * CHUNK,
            s1 * rows + (c0 + e) * CHUNK,
            (s0 + flip) * rows + c0 * CHUNK,
            (s1 + flip) * rows + (c0 + e) * CHUNK,
        )
        for i, start in enumerate(starts):
            at = pl.ds(pl.multiple_of(start, CHUNK), CHUNK)
            kout[at, :] = k[i * CHUNK : (i + 1) * CHUNK]
            vout[at, :] = v[i * CHUNK : (i + 1) * CHUNK]

    def near(g, carry):
        @pl.when(g < nchunk)
        def _():
            ship(g)

            @pl.when(g % 2 == 0)
            def _():
                forward(g, 0).start()

            @pl.when(g % 2 == 1)
            def _():
                forward(g, 1).start()

        @pl.when(g > 0)
        def _():
            arrive(g - 1)

        return carry

    lax.fori_loop(0, nchunk + 1, near, 0)

    for copy in cz_copies:
        copy.wait_recv()
    _, peak, later_z = scanned(czs, nz, z)
    later = later_x + later_z
    own_gate = ngate[t]
    own_forget = nforget[t]
    peak8 = jnp.concatenate([peak, peak], axis=0)
    stable = jnp.maximum(own_forget + peak8, own_gate)
    shift = own_forget - stable
    for s in range(2 * ntp):
        whole = wlog[s, 0:hd, :] + later
        cwout[:, s * 128 : (s + 1) * 128] = jnp.exp(whole - peak)
        wlog[s, 0:hd, :] = jnp.exp(whole + shift[0:hd])

    query = jnp.broadcast_to(nq[...], (2 * hd, nq.shape[1]))
    lane_head = lax.broadcasted_iota(jnp.int32, query.shape, 1) // DQK
    row_head = lax.broadcasted_iota(jnp.int32, query.shape, 0)
    queries = jnp.where(lane_head == row_head, query.astype(F32), 0.0)
    queries_low = queries.astype(BF16)
    acc[...] = jnp.zeros_like(acc)
    den[...] = jnp.zeros_like(den)

    def read(unit):
        at = pl.ds(pl.multiple_of(unit * 128, 128), 128)
        score = lax.dot_general(
            queries_low, kout[at, :], (((1,), (1,)), ((), ())), preferred_element_type=F32
        ) * (1.0 / math.sqrt(DQK))
        weighted = wlog[unit] * score
        den[...] += weighted
        acc[...] += jnp.dot(weighted.astype(BF16), vout[at, :], preferred_element_type=F32)

    def read_near(i, carry):
        away = (i // 4) + (i // 8)
        read(4 * ((t // 2 + away) % (ntp // 2)) + i % 4)
        return carry

    lax.fori_loop(0, 12, read_near, 0)

    def far(g, carry):
        @pl.when(g < nchunk + nchunk // 2)
        def _():
            ship(g)

        @pl.when(g > nchunk)
        def _():
            arrive(g - 1)

        return carry

    lax.fori_loop(nchunk, nchunk + nchunk // 2 + 1, far, 0)
    opposite = 4 * ((t // 2 + 2) % (ntp // 2))

    def read_far(i, carry):
        read(opposite + i)
        return carry

    lax.fori_loop(0, 4, read_far, 0)

    for h in range(hd):
        dpay[h : h + 1, :] = acc[h : h + 1, h * DV : (h + 1) * DV]
    dpay[hd : 2 * hd, :] = den[0:hd, :]
    dx_copies = across(lambda to: dpay, dxs, x, nx, "sp_1", dx_s, dx_r)
    dxs[x] = dpay[...]
    for copy in dx_copies:
        copy.wait_recv()
    drow[...] = functools.reduce(jnp.add, [dxs[s] for s in range(nx)])
    dz_copies = across(lambda to: drow, dzs, z, nz, "sp_0", dz_s, dz_r)
    dzs[z] = drow[...]
    for copy in dz_copies:
        copy.wait_recv()
    summed = functools.reduce(jnp.add, [dzs[s] for s in range(nz)])
    new_score = jnp.sum(
        queries * new_k[0:1, :].astype(F32), axis=1, keepdims=True
    )[0:hd] * (1.0 / math.sqrt(DQK))
    own_term = jnp.exp(own_gate - stable)[0:hd] * new_score
    values = jnp.concatenate(
        [new_v[0:1, h * DV : (h + 1) * DV].astype(F32) for h in range(hd)], axis=0
    )
    numerator = summed[0:hd] + own_term * values
    denominator = jnp.sum(summed[hd : 2 * hd], axis=1, keepdims=True) + own_term
    rdout[...] = numerator / jnp.maximum(jnp.abs(denominator), 1.0)

    def own_left(c, carry):
        for copy in own_copies(c):
            copy.wait_send()
        return carry

    lax.fori_loop(0, nchunk, own_left, 0)

    def forwards_left(i, carry):
        forward(2 * i, 0).wait_send()
        forward(2 * i + 1, 1).wait_send()
        return carry

    lax.fori_loop(0, nchunk // 2, forwards_left, 0)

    def sibling_left(g, carry):
        to_sibling(g).wait_send()
        return carry

    lax.fori_loop(0, nchunk + nchunk // 2, sibling_left, 0)
    own_to_sib.wait_send()
    for copy in (*b_copies, *cx_copies, *cz_copies, *dx_copies, *dz_copies):
        copy.wait_send()


def body(
    prompt_tokens,
    key_weight,
    value_weight,
    input_weight,
    forget_weight,
    forget_bias,
    new_token,
    new_query,
):
    nz, nx, ntp = (lax.axis_size(a) for a in ("sp_0", "sp_1", "tp"))
    rows, depth = prompt_tokens.shape
    kcols, vcols = key_weight.shape[1], value_weight.shape[1]
    heads = input_weight.shape[1]
    hd = heads // ntp
    assert hd == 4 and ntp == 8 and rows == 256
    nchunk = rows // CHUNK
    groups = nchunk + nchunk // 2
    anywhere = pl.BlockSpec(memory_space=pl.ANY)
    vmem = pl.BlockSpec(memory_space=pltpu.VMEM)
    dma = pltpu.SemaphoreType.DMA
    tile = (2 * hd, 128)
    key_cache, value_cache, cache_weight, reading = pl.pallas_call(
        kernel,
        out_shape=(
            jax.ShapeDtypeStruct((rows * ntp, kcols), BF16),
            jax.ShapeDtypeStruct((rows * ntp, vcols), BF16),
            jax.ShapeDtypeStruct((hd, rows * ntp), F32),
            jax.ShapeDtypeStruct((hd, DV), F32),
        ),
        in_specs=[anywhere] * 5 + [vmem] * 3,
        out_specs=[vmem] * 4,
        scratch_shapes=[
            pltpu.VMEM((rows, depth), BF16),
            pltpu.VMEM((rows, depth), BF16),
            pltpu.VMEM((groups, 4 * CHUNK, depth), BF16),
            pltpu.VMEM((depth, kcols), BF16),
            pltpu.VMEM((depth, vcols), BF16),
            pltpu.VMEM((depth, heads), BF16),
            pltpu.VMEM((depth, heads), BF16),
            pltpu.VMEM((ntp, 2 * hd, rows), F32),
            pltpu.VMEM((ntp, 2 * hd, rows), F32),
            pltpu.VMEM((ntp, *tile), F32),
            pltpu.VMEM((ntp, *tile), F32),
            pltpu.VMEM((2 * ntp, *tile), F32),
            pltpu.VMEM(tile, F32),
            pltpu.VMEM((nx, *tile), F32),
            pltpu.VMEM(tile, F32),
            pltpu.VMEM((nz, *tile), F32),
            pltpu.VMEM(tile, F32),
            pltpu.VMEM((nx, *tile), F32),
            pltpu.VMEM(tile, F32),
            pltpu.VMEM((nz, *tile), F32),
            pltpu.VMEM((2 * hd, vcols), F32),
            pltpu.VMEM(tile, F32),
            dma((5,)),
            dma((2, nchunk)),
            dma((2, groups)),
            dma((nchunk,)),
            dma((groups,)),
            dma((groups,)),
            dma(()),
            dma(()),
            dma((ntp - 1,)),
            dma((ntp - 1,)),
            dma((nx - 1,)),
            dma((nx - 1,)),
            dma((nz - 1,)),
            dma((nz - 1,)),
            dma((nx - 1,)),
            dma((nx - 1,)),
            dma((nz - 1,)),
            dma((nz - 1,)),
        ],
        compiler_params=pltpu.CompilerParams(
            collective_id=0, has_side_effects=True, vmem_limit_bytes=40 * 1024 * 1024
        ),
        name="prefill",
    )(
        prompt_tokens,
        key_weight,
        value_weight,
        input_weight,
        forget_weight,
        forget_bias.reshape(1, -1),
        new_token.reshape(1, -1),
        new_query.reshape(1, -1),
    )
    return key_cache, value_cache, cache_weight, reading.reshape(-1)


def solution(mesh):
    torus = Mesh(mesh.devices.reshape(8, 4, mesh.shape["tp"]), ("sp_0", "sp_1", "tp"))
    return jax.shard_map(
        body,
        mesh=torus,
        in_specs=(P(SP_TP, None), P(None, "tp"), P(None, "tp"), P(), P(), P(), P(), P("tp")),
        out_specs=(P(SP, "tp"), P(SP, "tp"), P("tp", SP), P("tp")),
        check_vma=False,
    )
```

```python
import functools
import math

import jax
import jax.numpy as jnp
from jax import lax
from jax.experimental import pallas as pl
from jax.experimental.pallas import tpu as pltpu
from jax.sharding import Mesh
from jax.sharding import PartitionSpec as P

DQK = 64
DV = 128
SP = ("sp_0", "sp_1")
SP_TP = ("sp_0", "sp_1", "tp")
MESH = pl.DeviceIdType.MESH
F32 = jnp.float32
BF16 = jnp.bfloat16
CHUNK = 32
EARLY = 3


def log_sigmoid(v):
    u = jnp.exp(-jnp.abs(v))
    w = 1.0 + u
    grown = w - 1.0
    tail = jnp.where(grown == 0.0, u, jnp.log(w) * (u / jnp.where(grown == 0.0, 1.0, grown)))
    return -(jnp.maximum(-v, 0.0) + tail)


def remote(src, dst, send, recv, where):
    return pltpu.make_async_remote_copy(
        src_ref=src, dst_ref=dst, send_sem=send, recv_sem=recv, device_id=where, device_id_type=MESH
    )


def kernel(
    tok, kw, vw, iw, fw, fb, nt, nq,
    kout, vout, cwout, rdout,
    xown, xsib, gat, wk, wv, wif, bias_v, token_v, query_v,
    sendb, recvb, ngate, nforget, wlog, cpay, cxs, crow, czs, dpay, dxs, drow, dzs, acc, den,
    lsem, own_s, own_r, fwd_s, sib_s, sib_r, osib_s, osib_r,
    b_s, b_r, cx_s, cx_r, cz_s, cz_r, dx_s, dx_r, dz_s, dz_r,
):
    nz, nx, ntp = (lax.axis_size(a) for a in ("sp_0", "sp_1", "tp"))
    z, x, t = (lax.axis_index(a) for a in ("sp_0", "sp_1", "tp"))
    flip = 1 - 2 * (t % 2)
    sib = t + flip
    up, dn = (t + 2) % ntp, (t + ntp - 2) % ntp
    rows = xown.shape[0]
    nchunk = rows // CHUNK

    loads = [
        pltpu.make_async_copy(src, dst, lsem.at[i])
        for i, (src, dst) in enumerate(
            (
                (tok, xown),
                (iw, wif.at[pl.ds(0, iw.shape[0])]),
                (fw, wif.at[pl.ds(iw.shape[0], iw.shape[0])]),
                (fb, bias_v),
                (nt, token_v),
                (nq, query_v),
                (kw, wk),
                (vw, wv),
            )
        )
    ]
    for load in loads:
        load.start()

    barrier = pltpu.get_barrier_semaphore()
    for axis, here, size in (("tp", t, ntp), ("sp_1", x, nx), ("sp_0", z, nz)):
        for d in range(1, size):
            pl.semaphore_signal(
                barrier, inc=1, device_id={axis: (here + d) % size}, device_id_type=MESH
            )
    pl.semaphore_wait(barrier, ntp + nx + nz - 3)

    def own_copies(c):
        piece = xown.at[pl.ds(c * CHUNK, CHUNK)]
        return (
            remote(piece, gat.at[c, pl.ds(0, CHUNK)], own_s.at[0, c], own_r.at[0, c], {"tp": up}),
            remote(
                piece, gat.at[c, pl.ds(CHUNK, CHUNK)], own_s.at[1, c], own_r.at[1, c], {"tp": dn}
            ),
        )

    def send_own(c, carry):
        for copy in own_copies(c):
            copy.start()
        return carry

    def to_sibling(g):
        return remote(
            gat.at[g, pl.ds(0, 2 * CHUNK)],
            gat.at[g, pl.ds(2 * CHUNK, 2 * CHUNK)],
            sib_s.at[g],
            sib_r.at[g],
            {"tp": sib},
        )

    loads[0].wait()
    lax.fori_loop(0, EARLY, send_own, 0)
    own_to_sib = remote(xown, xsib, osib_s, osib_r, {"tp": sib})
    own_to_sib.start()

    for load in loads[1:6]:
        load.wait()
    heads = iw.shape[0]
    hd = heads // ntp
    depth = xown.shape[1]
    bias = bias_v[...].reshape(1, heads).T
    token16 = jnp.broadcast_to(token_v[...].reshape(1, depth), (16, depth))
    over_lanes = (((1,), (1,)), ((), ()))
    gates = lax.dot_general(wif[...], xown[...], over_lanes, preferred_element_type=F32)
    gate_t = gates[0:heads]
    forget_t = log_sigmoid(gates[heads:] + bias)
    later_mask = (
        lax.broadcasted_iota(jnp.int32, (rows, rows), 0)
        > lax.broadcasted_iota(jnp.int32, (rows, rows), 1)
    ).astype(F32).astype(BF16)
    high = forget_t.astype(BF16)
    rest = forget_t - high.astype(F32)
    mid = rest.astype(BF16)
    low = (rest - mid.astype(F32)).astype(BF16)
    suffix = (
        jnp.dot(low, later_mask, preferred_element_type=F32)
        + jnp.dot(mid, later_mask, preferred_element_type=F32)
        + jnp.dot(high, later_mask, preferred_element_type=F32)
    )
    logw = gate_t + suffix
    total = jnp.broadcast_to(suffix[:, 0:1] + forget_t[:, 0:1], (heads, rows))
    new_gates = lax.dot_general(wif[...], token16, over_lanes, preferred_element_type=F32)
    new_gt = jnp.broadcast_to(new_gates[0:heads, 0:1], (heads, 128))
    new_ft = jnp.broadcast_to(log_sigmoid(new_gates[heads:, 0:1] + bias), (heads, 128))
    for j in range(ntp):
        pick = slice(j * hd, (j + 1) * hd)
        sendb[j, 0:hd, :] = logw[pick]
        sendb[j, hd : 2 * hd, :] = total[pick]
        ngate[j, 0:hd, :] = new_gt[pick]
        ngate[j, hd : 2 * hd, :] = new_gt[pick]
        nforget[j, 0:hd, :] = new_ft[pick]
        nforget[j, hd : 2 * hd, :] = new_ft[pick]

    def across(src, dst_slots, here, size, axis, send, recv):
        copies = []
        for d in range(1, size):
            to = (here + d) % size
            copies.append(
                remote(src(to), dst_slots.at[here], send.at[d - 1], recv.at[d - 1], {axis: to})
            )
        for copy in copies:
            copy.start()
        return copies

    b_copies = across(lambda to: sendb.at[to], recvb, t, ntp, "tp", b_s, b_r)
    recvb[t] = sendb[t]
    lax.fori_loop(EARLY, nchunk, send_own, 0)

    def project(lhs):
        k = jnp.dot(lhs, wk[...], preferred_element_type=F32).astype(BF16)
        v = jnp.dot(lhs, wv[...], preferred_element_type=F32).astype(BF16)
        return k, v

    loads[6].wait()
    loads[7].wait()
    new_k, new_v = project(token16)

    def whole_block(src, source):
        k, v = project(src[...])
        at = pl.ds(pl.multiple_of(source * rows, rows), rows)
        kout[at, :] = k
        vout[at, :] = v

    whole_block(xown, t)

    for copy in b_copies:
        copy.wait_recv()
    zero = jnp.zeros((hd, 128), F32)
    later = zero
    best = None
    for s in reversed(range(ntp)):
        tile = recvb[s]
        for half in (1, 0):
            part = tile[0:hd, half * 128 : (half + 1) * 128] + later
            wlog[2 * s + half, 0:hd, :] = part
            wlog[2 * s + half, hd : 2 * hd, :] = zero
            best = part if best is None else jnp.maximum(best, part)
        later = later + tile[hd : 2 * hd, 0:128]
    block_peak = jnp.broadcast_to(jnp.max(best, axis=1, keepdims=True), (hd, 128))
    cpay[0:hd, :] = later
    cpay[hd : 2 * hd, :] = block_peak
    cx_copies = across(lambda to: cpay, cxs, x, nx, "sp_1", cx_s, cx_r)
    cxs[x] = cpay[...]

    own_to_sib.wait_recv()
    whole_block(xsib, sib)

    for copy in cx_copies:
        copy.wait_recv()

    def scanned(slots, size, here):
        behind = zero
        mine = zero
        peak = None
        for s in reversed(range(size)):
            tile = slots[s]
            candidate = tile[hd : 2 * hd] + behind
            peak = candidate if peak is None else jnp.maximum(peak, candidate)
            mine = mine + jnp.where(s > here, tile[0:hd], zero)
            behind = behind + tile[0:hd]
        return behind, peak, mine

    row_total, row_peak, later_x = scanned(cxs, nx, x)
    crow[0:hd, :] = row_total
    crow[hd : 2 * hd, :] = row_peak
    cz_copies = across(lambda to: crow, czs, z, nz, "sp_0", cz_s, cz_r)
    czs[z] = crow[...]

    def ship(g):
        pltpu.make_async_copy(gat.at[g, pl.ds(0, CHUNK)], gat.at[g, pl.ds(0, CHUNK)], own_r.at[0, g]).wait()
        pltpu.make_async_copy(gat.at[g, pl.ds(0, CHUNK)], gat.at[g, pl.ds(0, CHUNK)], own_r.at[1, g]).wait()
        to_sibling(g).start()

    def forward(g, side):
        half = pl.ds(side * CHUNK, CHUNK)
        return remote(
            gat.at[g, half],
            gat.at[nchunk + g // 2, half],
            fwd_s.at[g],
            own_r.at[side, nchunk + g // 2],
            {"tp": dn if side else up},
        )

    def arrive(g):
        pltpu.make_async_copy(
            gat.at[g, pl.ds(0, 2 * CHUNK)], gat.at[g, pl.ds(0, 2 * CHUNK)], sib_r.at[g]
        ).wait()
        k, v = project(gat[g])
        e = g // nchunk
        c0 = g + e * (g - 2 * nchunk)
        s0 = (t + ntp - 2 - 2 * e) % ntp
        s1 = (t + 2 + 2 * e) % ntp
        starts = (
            s0 * rows + c0 * CHUNK,
            s1 * rows + (c0 + e) * CHUNK,
            (s0 + flip) * rows + c0 * CHUNK,
            (s1 + flip) * rows + (c0 + e) * CHUNK,
        )
        for i, start in enumerate(starts):
            at = pl.ds(pl.multiple_of(start, CHUNK), CHUNK)
            kout[at, :] = k[i * CHUNK : (i + 1) * CHUNK]
            vout[at, :] = v[i * CHUNK : (i + 1) * CHUNK]

    def near(g, carry):
        @pl.when(g < nchunk)
        def _():
            ship(g)

            @pl.when(g % 2 == 0)
            def _():
                forward(g, 0).start()

            @pl.when(g % 2 == 1)
            def _():
                forward(g, 1).start()

        @pl.when(g > 0)
        def _():
            arrive(g - 1)

        return carry

    lax.fori_loop(0, nchunk + 1, near, 0)

    for copy in cz_copies:
        copy.wait_recv()
    _, peak, later_z = scanned(czs, nz, z)
    later = later_x + later_z
    own_gate = ngate[t]
    own_forget = nforget[t]
    peak8 = jnp.concatenate([peak, peak], axis=0)
    stable = jnp.maximum(own_forget + peak8, own_gate)
    shift = own_forget - stable
    for s in range(2 * ntp):
        whole = wlog[s, 0:hd, :] + later
        cwout[:, s * 128 : (s + 1) * 128] = jnp.exp(whole - peak)
        wlog[s, 0:hd, :] = jnp.exp(whole + shift[0:hd])

    query = jnp.broadcast_to(query_v[...].reshape(1, -1), (2 * hd, nq.shape[0]))
    lane_head = lax.broadcasted_iota(jnp.int32, query.shape, 1) // DQK
    row_head = lax.broadcasted_iota(jnp.int32, query.shape, 0)
    queries = jnp.where(lane_head == row_head, query.astype(F32), 0.0)
    queries_low = queries.astype(BF16)
    acc[...] = jnp.zeros_like(acc)
    den[...] = jnp.zeros_like(den)

    def read(unit):
        at = pl.ds(pl.multiple_of(unit * 128, 128), 128)
        score = lax.dot_general(
            queries_low, kout[at, :], (((1,), (1,)), ((), ())), preferred_element_type=F32
        ) * (1.0 / math.sqrt(DQK))
        weighted = wlog[unit] * score
        den[...] += weighted
        acc[...] += jnp.dot(weighted.astype(BF16), vout[at, :], preferred_element_type=F32)

    def read_near(i, carry):
        away = (i // 4) + (i // 8)
        read(4 * ((t // 2 + away) % (ntp // 2)) + i % 4)
        return carry

    lax.fori_loop(0, 12, read_near, 0)

    def far(g, carry):
        @pl.when(g < nchunk + nchunk // 2)
        def _():
            ship(g)

        @pl.when(g > nchunk)
        def _():
            arrive(g - 1)

        return carry

    lax.fori_loop(nchunk, nchunk + nchunk // 2 + 1, far, 0)
    opposite = 4 * ((t // 2 + 2) % (ntp // 2))

    def read_far(i, carry):
        read(opposite + i)
        return carry

    lax.fori_loop(0, 4, read_far, 0)

    for h in range(hd):
        dpay[h : h + 1, :] = acc[h : h + 1, h * DV : (h + 1) * DV]
    dpay[hd : 2 * hd, :] = den[0:hd, :]
    dx_copies = across(lambda to: dpay, dxs, x, nx, "sp_1", dx_s, dx_r)
    dxs[x] = dpay[...]
    for copy in dx_copies:
        copy.wait_recv()
    drow[...] = functools.reduce(jnp.add, [dxs[s] for s in range(nx)])
    dz_copies = across(lambda to: drow, dzs, z, nz, "sp_0", dz_s, dz_r)
    dzs[z] = drow[...]
    for copy in dz_copies:
        copy.wait_recv()
    summed = functools.reduce(jnp.add, [dzs[s] for s in range(nz)])
    new_score = jnp.sum(
        queries * new_k[0:1, :].astype(F32), axis=1, keepdims=True
    )[0:hd] * (1.0 / math.sqrt(DQK))
    own_term = jnp.exp(own_gate - stable)[0:hd] * new_score
    values = jnp.concatenate(
        [new_v[0:1, h * DV : (h + 1) * DV].astype(F32) for h in range(hd)], axis=0
    )
    numerator = summed[0:hd] + own_term * values
    denominator = jnp.sum(summed[hd : 2 * hd], axis=1, keepdims=True) + own_term
    rdout[...] = numerator / jnp.maximum(jnp.abs(denominator), 1.0)

    def own_left(c, carry):
        for copy in own_copies(c):
            copy.wait_send()
        return carry

    lax.fori_loop(0, nchunk, own_left, 0)

    def forwards_left(i, carry):
        forward(2 * i, 0).wait_send()
        forward(2 * i + 1, 1).wait_send()
        return carry

    lax.fori_loop(0, nchunk // 2, forwards_left, 0)

    def sibling_left(g, carry):
        to_sibling(g).wait_send()
        return carry

    lax.fori_loop(0, nchunk + nchunk // 2, sibling_left, 0)
    own_to_sib.wait_send()
    for copy in (*b_copies, *cx_copies, *cz_copies, *dx_copies, *dz_copies):
        copy.wait_send()


def put_out(*refs):
    sems = refs[8]
    copies = [pltpu.make_async_copy(refs[i], refs[4 + i], sems.at[i]) for i in range(4)]
    for copy in copies:
        copy.start()
    for copy in copies:
        copy.wait()


def body(
    prompt_tokens,
    key_weight,
    value_weight,
    input_weight,
    forget_weight,
    forget_bias,
    new_token,
    new_query,
):
    nz, nx, ntp = (lax.axis_size(a) for a in ("sp_0", "sp_1", "tp"))
    rows, depth = prompt_tokens.shape
    kcols, vcols = key_weight.shape[1], value_weight.shape[1]
    heads = input_weight.shape[1]
    hd = heads // ntp
    assert hd == 4 and ntp == 8 and rows == 256
    nchunk = rows // CHUNK
    groups = nchunk + nchunk // 2
    anywhere = pl.BlockSpec(memory_space=pltpu.HBM)
    vmem = pl.BlockSpec(memory_space=pltpu.VMEM)
    dma = pltpu.SemaphoreType.DMA
    tile = (2 * hd, 128)
    key_cache, value_cache, cache_weight, reading = pl.pallas_call(
        kernel,
        out_shape=(
            jax.ShapeDtypeStruct((rows * ntp, kcols), BF16),
            jax.ShapeDtypeStruct((rows * ntp, vcols), BF16),
            jax.ShapeDtypeStruct((hd, rows * ntp), F32),
            jax.ShapeDtypeStruct((hd, DV), F32),
        ),
        in_specs=[anywhere] * 8,
        out_specs=[vmem] * 4,
        scratch_shapes=[
            pltpu.VMEM((rows, depth), BF16),
            pltpu.VMEM((rows, depth), BF16),
            pltpu.VMEM((groups, 4 * CHUNK, depth), BF16),
            pltpu.VMEM((depth, kcols), BF16),
            pltpu.VMEM((depth, vcols), BF16),
            pltpu.VMEM((2 * heads, depth), BF16),
            pltpu.VMEM((heads,), F32),
            pltpu.VMEM((depth,), BF16),
            pltpu.VMEM((kcols,), BF16),
            pltpu.VMEM((ntp, 2 * hd, rows), F32),
            pltpu.VMEM((ntp, 2 * hd, rows), F32),
            pltpu.VMEM((ntp, *tile), F32),
            pltpu.VMEM((ntp, *tile), F32),
            pltpu.VMEM((2 * ntp, *tile), F32),
            pltpu.VMEM(tile, F32),
            pltpu.VMEM((nx, *tile), F32),
            pltpu.VMEM(tile, F32),
            pltpu.VMEM((nz, *tile), F32),
            pltpu.VMEM(tile, F32),
            pltpu.VMEM((nx, *tile), F32),
            pltpu.VMEM(tile, F32),
            pltpu.VMEM((nz, *tile), F32),
            pltpu.VMEM((2 * hd, vcols), F32),
            pltpu.VMEM(tile, F32),
            dma((8,)),
            dma((2, nchunk)),
            dma((2, groups)),
            dma((nchunk,)),
            dma((groups,)),
            dma((groups,)),
            dma(()),
            dma(()),
            dma((ntp - 1,)),
            dma((ntp - 1,)),
            dma((nx - 1,)),
            dma((nx - 1,)),
            dma((nz - 1,)),
            dma((nz - 1,)),
            dma((nx - 1,)),
            dma((nx - 1,)),
            dma((nz - 1,)),
            dma((nz - 1,)),
        ],
        compiler_params=pltpu.CompilerParams(
            collective_id=0, has_side_effects=True, vmem_limit_bytes=40 * 1024 * 1024
        ),
        name="prefill",
    )(
        *(
            pltpu.with_memory_space_constraint(operand, pltpu.HBM)
            for operand in (
                prompt_tokens,
                key_weight,
                value_weight,
                input_weight.T,
                forget_weight.T,
                forget_bias,
                new_token,
                new_query,
            )
        )
    )
    results = (key_cache, value_cache, cache_weight, reading)
    key_cache, value_cache, cache_weight, reading = pl.pallas_call(
        put_out,
        out_shape=tuple(jax.ShapeDtypeStruct(r.shape, r.dtype) for r in results),
        in_specs=[vmem] * 4,
        out_specs=[anywhere] * 4,
        scratch_shapes=[dma((4,))],
        compiler_params=pltpu.CompilerParams(vmem_limit_bytes=1024 * 1024),
        name="put_out",
    )(*results)
    return key_cache, value_cache, cache_weight, reading.reshape(-1)


def solution(mesh):
    torus = Mesh(mesh.devices.reshape(8, 4, mesh.shape["tp"]), ("sp_0", "sp_1", "tp"))
    return jax.shard_map(
        body,
        mesh=torus,
        in_specs=(P(SP_TP, None), P(None, "tp"), P(None, "tp"), P(), P(), P(), P(), P("tp")),
        out_specs=(P(SP, "tp"), P(SP, "tp"), P("tp", SP), P("tp")),
        check_vma=False,
    )
```

```python
import functools
import math

import jax
import jax.numpy as jnp
from jax import lax
from jax.experimental import pallas as pl
from jax.experimental.pallas import tpu as pltpu
from jax.sharding import Mesh
from jax.sharding import PartitionSpec as P

DQK = 64
DV = 128
SP = ("sp_0", "sp_1")
SP_TP = ("sp_0", "sp_1", "tp")
MESH = pl.DeviceIdType.MESH
F32 = jnp.float32
BF16 = jnp.bfloat16
CHUNK = 32
EARLY = (2, 4)


def log_sigmoid(v):
    u = jnp.exp(-jnp.abs(v))
    w = 1.0 + u
    grown = w - 1.0
    tail = jnp.where(grown == 0.0, u, jnp.log(w) * (u / jnp.where(grown == 0.0, 1.0, grown)))
    return -(jnp.maximum(-v, 0.0) + tail)


def remote(src, dst, send, recv, where):
    return pltpu.make_async_remote_copy(
        src_ref=src, dst_ref=dst, send_sem=send, recv_sem=recv, device_id=where, device_id_type=MESH
    )


def kernel(
    tok, kw, vw, iw, fw, fb, nt, nq,
    kout, vout, cwout, rdout,
    xown, xsib, gat, wk, wv, wif, bias_v, token_v, query_v,
    tmrow, tmall, lwpay, lwall, wread, cpay, cxs, crow, czs, dpay, dxs, drow, dzs, acc, den,
    lsem, own_s, own_r, fwd_s, sib_s, sib_r, osib_s, osib_r,
    tm_s, tm_r, lw_s, lw_r, cx_s, cx_r, cz_s, cz_r, dx_s, dx_r, dz_s, dz_r, near_z,
):
    nz, nx, ntp = (lax.axis_size(a) for a in ("sp_0", "sp_1", "tp"))
    z, x, t = (lax.axis_index(a) for a in ("sp_0", "sp_1", "tp"))
    flip = 1 - 2 * (t % 2)
    sib = t + flip
    up, dn = (t + 2) % ntp, (t + ntp - 2) % ntp
    rows, depth = xown.shape
    nchunk = rows // CHUNK
    groups = gat.shape[0]
    heads = iw.shape[0]
    hd = heads // ntp
    over_lanes = (((1,), (1,)), ((), ()))

    loads = [
        pltpu.make_async_copy(src, dst, lsem.at[i])
        for i, (src, dst) in enumerate(
            (
                (tok, xown),
                (iw, wif.at[pl.ds(0, heads)]),
                (fw, wif.at[pl.ds(heads, heads)]),
                (fb, bias_v),
                (nt, token_v),
                (nq, query_v),
                (kw, wk),
                (vw, wv),
            )
        )
    ]
    for load in loads:
        load.start()

    barrier = pltpu.get_barrier_semaphore()

    def signal(semaphore, axis, to):
        pl.semaphore_signal(semaphore, inc=1, device_id={axis: to}, device_id_type=MESH)

    for d in range(1, ntp):
        signal(barrier, "tp", (t + d) % ntp)
    for d in range(1, nx):
        signal(barrier, "sp_1", (x + d) % nx)
    for d in (1, nz - 1):
        signal(barrier, "sp_0", (z + d) % nz)
    pl.semaphore_wait(barrier, ntp + nx)
    for d in (1, nz - 1):
        signal(near_z.at[0], "sp_0", (z + d) % nz)

    def own_copies(c):
        piece = xown.at[pl.ds(c * CHUNK, CHUNK)]
        return (
            remote(piece, gat.at[c, pl.ds(0, CHUNK)], own_s.at[0, c], own_r.at[0, c], {"tp": up}),
            remote(
                piece, gat.at[c, pl.ds(CHUNK, CHUNK)], own_s.at[1, c], own_r.at[1, c], {"tp": dn}
            ),
        )

    def send_own(c, carry):
        for copy in own_copies(c):
            copy.start()
        return carry

    def across(src, dst_slots, here, size, axis, send, recv):
        copies = []
        for d in range(1, size):
            to = (here + d) % size
            copies.append(
                remote(src(to), dst_slots.at[here], send.at[d - 1], recv.at[d - 1], {axis: to})
            )
        for copy in copies:
            copy.start()
        return copies

    loads[0].wait()
    lax.fori_loop(0, EARLY[0], send_own, 0)
    own_to_sib = remote(xown, xsib, osib_s, osib_r, {"tp": sib})
    own_to_sib.start()

    for load in loads[1:6]:
        load.wait()
    bias = bias_v[...].reshape(1, heads).T
    gates = lax.dot_general(wif[...], xown[...], over_lanes, preferred_element_type=F32)
    gate_t = gates[0:heads]
    forget_t = log_sigmoid(gates[heads:] + bias)
    later_mask = (
        lax.broadcasted_iota(jnp.int32, (rows, rows), 0)
        > lax.broadcasted_iota(jnp.int32, (rows, rows), 1)
    ).astype(F32).astype(BF16)
    high = forget_t.astype(BF16)
    rest = forget_t - high.astype(F32)
    mid = rest.astype(BF16)
    low = (rest - mid.astype(F32)).astype(BF16)
    suffix = (
        jnp.dot(low, later_mask, preferred_element_type=F32)
        + jnp.dot(mid, later_mask, preferred_element_type=F32)
        + jnp.dot(high, later_mask, preferred_element_type=F32)
    )
    logw = gate_t + suffix
    total = suffix[:, 0:1] + forget_t[:, 0:1]
    top = jnp.max(logw, axis=1, keepdims=True)
    lane = lax.broadcasted_iota(jnp.int32, (heads, 128), 1)
    pairs = jnp.concatenate(
        [jnp.where(lane < 64, total, top), jnp.zeros((128 - heads, 128), F32)], axis=0
    ).T
    tmrow[0:1, :] = pairs[0:1]
    tmrow[1:2, :] = pairs[64:65]
    tm_copies = across(lambda to: tmrow, tmall, t, ntp, "tp", tm_s, tm_r)
    tmall[t] = tmrow[...]

    lax.fori_loop(EARLY[0], EARLY[1], send_own, 0)

    pl.semaphore_wait(near_z.at[0], 2)
    for d in (2, nz - 2):
        signal(near_z.at[1], "sp_0", (z + d) % nz)

    def project(lhs):
        k = jnp.dot(lhs, wk[...], preferred_element_type=F32).astype(BF16)
        v = jnp.dot(lhs, wv[...], preferred_element_type=F32).astype(BF16)
        return k, v

    def whole_block(src, source):
        k, v = project(src[...])
        at = pl.ds(pl.multiple_of(source * rows, rows), rows)
        kout[at, :] = k
        vout[at, :] = v

    loads[6].wait()
    loads[7].wait()
    whole_block(xown, t)

    for copy in tm_copies:
        copy.wait_recv()
    block_total = jnp.zeros((1, 128), F32)
    mine = block_total
    block_top = None
    for s in reversed(range(ntp)):
        candidate = tmall[s, 1:2, :] + block_total
        block_top = candidate if block_top is None else jnp.maximum(block_top, candidate)
        mine = mine + jnp.where(s > t, tmall[s, 0:1, :], 0.0)
        block_total = block_total + tmall[s, 0:1, :]
    logw = logw + mine.T[0:heads]

    def twice(a):
        return jnp.concatenate(
            [a[j * hd : (j + 1) * hd] for j in range(ntp) for _ in (0, 1)], axis=0
        )

    def is_first(width):
        return lax.broadcasted_iota(jnp.int32, (2 * heads, width), 0) % (2 * hd) < hd

    logw2 = twice(logw)
    packed = jnp.where(is_first(128), logw2[:, :128], logw2[:, 128:])
    for j in range(ntp):
        lwpay[j] = packed[j * 2 * hd : (j + 1) * 2 * hd]
    lw_copies = across(lambda to: lwpay.at[to], lwall, t, ntp, "tp", lw_s, lw_r)
    lwall[t] = lwpay[t]

    lax.fori_loop(EARLY[1], nchunk, send_own, 0)

    token16 = jnp.broadcast_to(token_v[...].reshape(1, depth), (16, depth))
    new_k, new_v = project(token16)
    new_gates = lax.dot_general(wif[...], token16, over_lanes, preferred_element_type=F32)[:, 0:1]
    own_lane = lax.broadcasted_iota(jnp.int32, (hd, 128), 1)
    own_row = lax.broadcasted_iota(jnp.int32, (hd, 128), 0)
    own_pick = own_lane == t * hd + own_row

    def own_heads(row):
        column = jnp.sum(jnp.where(own_pick, row, 0.0), axis=1, keepdims=True)
        return jnp.broadcast_to(column, (hd, 128))

    own_head_col = (
        lax.broadcasted_iota(jnp.int32, (heads, hd), 0)
        == t * hd + lax.broadcasted_iota(jnp.int32, (heads, hd), 1)
    )

    def own_columns(column):
        row = jnp.sum(jnp.where(own_head_col, column, 0.0), axis=0, keepdims=True)
        return jnp.broadcast_to(row.T, (hd, 128))

    new_gate = own_columns(new_gates[0:heads])
    new_forget = own_columns(log_sigmoid(new_gates[heads:] + bias))

    cpay[0:hd, :] = own_heads(block_total)
    cpay[hd:, :] = own_heads(block_top)
    cx_copies = across(lambda to: cpay, cxs, x, nx, "sp_1", cx_s, cx_r)
    cxs[x] = cpay[...]

    own_to_sib.wait_recv()
    whole_block(xsib, sib)

    def scanned(slots, size, here):
        behind = jnp.zeros((hd, 128), F32)
        mine = behind
        peak = None
        for s in reversed(range(size)):
            level = slots[s, hd:, :] + behind
            peak = level if peak is None else jnp.maximum(peak, level)
            mine = mine + jnp.where(s > here, slots[s, 0:hd, :], 0.0)
            behind = behind + slots[s, 0:hd, :]
        return behind, peak, mine

    def landed(ref, semaphore):
        pltpu.make_async_copy(ref, ref, semaphore).wait()

    def to_sibling(g):
        return remote(
            gat.at[g, pl.ds(0, 2 * CHUNK)],
            gat.at[g, pl.ds(2 * CHUNK, 2 * CHUNK)],
            sib_s.at[g],
            sib_r.at[g],
            {"tp": sib},
        )

    def ship(g):
        landed(gat.at[g, pl.ds(0, CHUNK)], own_r.at[0, g])
        landed(gat.at[g, pl.ds(CHUNK, CHUNK)], own_r.at[1, g])
        to_sibling(g).start()

    def forward(g, side):
        part = pl.ds(side * CHUNK, CHUNK)
        return remote(
            gat.at[g, part],
            gat.at[nchunk + g // 2, part],
            fwd_s.at[g],
            own_r.at[side, nchunk + g // 2],
            {"tp": dn if side else up},
        )

    def pieces(g):
        e = g // nchunk
        c0 = g + e * (g - 2 * nchunk)
        s0 = (t + ntp - 2 - 2 * e) % ntp
        s1 = (t + 2 + 2 * e) % ntp
        return (
            s0 * rows + c0 * CHUNK,
            s1 * rows + (c0 + e) * CHUNK,
            (s0 + flip) * rows + c0 * CHUNK,
            (s1 + flip) * rows + (c0 + e) * CHUNK,
        )

    def place(lhs, starts):
        k, v = project(lhs)
        for i, start in enumerate(starts):
            at = pl.ds(pl.multiple_of(start, CHUNK), CHUNK)
            kout[at, :] = k[i * CHUNK : (i + 1) * CHUNK]
            vout[at, :] = v[i * CHUNK : (i + 1) * CHUNK]

    def from_sibling(g):
        landed(gat.at[g, pl.ds(2 * CHUNK, 2 * CHUNK)], sib_r.at[g])

    def arrive(g):
        from_sibling(g)
        place(gat[g], pieces(g))

    def near(g, carry):
        ship(g)

        @pl.when(g % 2 == 0)
        def _():
            forward(g, 0).start()

        @pl.when(g % 2 == 1)
        def _():
            forward(g, 1).start()

        @pl.when(g > 0)
        def _():
            arrive(g - 1)

        return carry

    lax.fori_loop(0, nchunk // 2, near, 0)
    for copy in cx_copies:
        copy.wait_recv()
    row_total, row_peak, later_x = scanned(cxs, nx, x)
    crow[0:hd, :] = row_total
    crow[hd:, :] = row_peak
    pl.semaphore_wait(near_z.at[1], 2)
    cz_copies = across(lambda to: crow, czs, z, nz, "sp_0", cz_s, cz_r)
    czs[z] = crow[...]
    lax.fori_loop(nchunk // 2, nchunk, near, 0)

    for copy in (*cz_copies, *lw_copies):
        copy.wait_recv()
    _, peak, later_z = scanned(czs, nz, z)
    later = later_x + later_z
    later2 = jnp.concatenate([later, later], axis=0)
    peak2 = jnp.concatenate([peak, peak], axis=0)
    stable = jnp.maximum(new_forget + peak, new_gate)
    shift = new_forget - stable
    shift2 = jnp.concatenate([shift, shift], axis=0)
    zero = jnp.zeros((hd, 128), F32)
    for s in range(ntp):
        whole = lwall[s] + later2
        tile = jnp.exp(whole - peak2)
        cwout[:, s * rows : s * rows + 128] = tile[0:hd]
        cwout[:, s * rows + 128 : (s + 1) * rows] = tile[hd:]
        tile = jnp.exp(whole + shift2)
        wread[2 * s] = jnp.concatenate([tile[0:hd], zero], axis=0)
        wread[2 * s + 1] = jnp.concatenate([tile[hd:], zero], axis=0)

    query = jnp.broadcast_to(query_v[...].reshape(1, -1), (2 * hd, nq.shape[0])).astype(F32)
    lane_head = lax.broadcasted_iota(jnp.int32, query.shape, 1) // DQK
    row_head = lax.broadcasted_iota(jnp.int32, query.shape, 0)
    queries = jnp.where(lane_head == row_head, query, 0.0)
    queries_low = queries.astype(BF16)
    acc[...] = jnp.zeros_like(acc)
    den[...] = jnp.zeros_like(den)

    def read(unit):
        at = pl.ds(pl.multiple_of(unit * 128, 128), 128)
        score = lax.dot_general(
            queries_low, kout[at, :], over_lanes, preferred_element_type=F32
        ) * (1.0 / math.sqrt(DQK))
        weighted = wread[unit] * score
        den[...] += weighted
        acc[...] += jnp.dot(weighted.astype(BF16), vout[at, :], preferred_element_type=F32)

    opposite = 4 * ((t // 2 + 2) % (ntp // 2))
    ship(nchunk)
    arrive(nchunk - 1)

    def read_near(i, carry):
        away = (i // 4) + (i // 8)
        read(4 * ((t // 2 + away) % (ntp // 2)) + i % 4)
        return carry

    lax.fori_loop(0, 12, read_near, 0)

    def far(g, carry):
        ship(g)
        arrive(g - 1)
        return carry

    lax.fori_loop(nchunk + 1, groups - 1, far, 0)
    read(opposite)
    read(opposite + 2)
    last = groups - 1
    arrive(last - 1)
    ship(last)
    ends = pieces(last)
    place(gat[last, 0 : 2 * CHUNK], ends[0:2])
    from_sibling(last)
    place(gat[last, 2 * CHUNK :], ends[2:])
    read(opposite + 1)
    read(opposite + 3)

    for h in range(hd):
        dpay[h : h + 1, :] = acc[h : h + 1, h * DV : (h + 1) * DV]
    dpay[hd:, :] = den[0:hd, :]
    dx_copies = across(lambda to: dpay, dxs, x, nx, "sp_1", dx_s, dx_r)
    dxs[x] = dpay[...]
    new_score = jnp.sum(
        queries[0:hd] * new_k[0:1, :].astype(F32), axis=1, keepdims=True
    ) * (1.0 / math.sqrt(DQK))
    own_term = jnp.exp(new_gate - stable) * new_score
    values = jnp.concatenate(
        [new_v[0:1, h * DV : (h + 1) * DV].astype(F32) for h in range(hd)], axis=0
    )
    for copy in dx_copies:
        copy.wait_recv()
    drow[...] = functools.reduce(jnp.add, [dxs[s] for s in range(nx)])
    dz_copies = across(lambda to: drow, dzs, z, nz, "sp_0", dz_s, dz_r)
    dzs[z] = drow[...]
    for copy in dz_copies:
        copy.wait_recv()
    summed = functools.reduce(jnp.add, [dzs[s] for s in range(nz)])
    numerator = summed[0:hd] + own_term * values
    denominator = jnp.sum(summed[hd:], axis=1, keepdims=True) + own_term
    rdout[...] = numerator / jnp.maximum(jnp.abs(denominator), 1.0)

    def own_left(c, carry):
        for copy in own_copies(c):
            copy.wait_send()
        return carry

    lax.fori_loop(0, nchunk, own_left, 0)

    def forwards_left(i, carry):
        forward(2 * i, 0).wait_send()
        forward(2 * i + 1, 1).wait_send()
        return carry

    lax.fori_loop(0, nchunk // 2, forwards_left, 0)

    def sibling_left(g, carry):
        to_sibling(g).wait_send()
        return carry

    lax.fori_loop(0, groups, sibling_left, 0)
    own_to_sib.wait_send()
    for copy in (*tm_copies, *lw_copies, *cx_copies, *cz_copies, *dx_copies, *dz_copies):
        copy.wait_send()


def put_out(*refs):
    sems = refs[8]
    copies = [pltpu.make_async_copy(refs[i], refs[4 + i], sems.at[i]) for i in range(4)]
    for copy in copies:
        copy.start()
    for copy in copies:
        copy.wait()


def body(
    prompt_tokens,
    key_weight,
    value_weight,
    input_weight,
    forget_weight,
    forget_bias,
    new_token,
    new_query,
):
    nz, nx, ntp = (lax.axis_size(a) for a in ("sp_0", "sp_1", "tp"))
    rows, depth = prompt_tokens.shape
    kcols, vcols = key_weight.shape[1], value_weight.shape[1]
    heads = input_weight.shape[1]
    hd = heads // ntp
    assert hd == 4 and ntp == 8 and rows == 256
    nchunk = rows // CHUNK
    groups = nchunk + nchunk // 2
    anywhere = pl.BlockSpec(memory_space=pltpu.HBM)
    vmem = pl.BlockSpec(memory_space=pltpu.VMEM)
    dma = pltpu.SemaphoreType.DMA
    tile = (2 * hd, 128)
    key_cache, value_cache, cache_weight, reading = pl.pallas_call(
        kernel,
        out_shape=(
            jax.ShapeDtypeStruct((rows * ntp, kcols), BF16),
            jax.ShapeDtypeStruct((rows * ntp, vcols), BF16),
            jax.ShapeDtypeStruct((hd, rows * ntp), F32),
            jax.ShapeDtypeStruct((hd, DV), F32),
        ),
        in_specs=[anywhere] * 8,
        out_specs=[vmem] * 4,
        scratch_shapes=[
            pltpu.VMEM((rows, depth), BF16),
            pltpu.VMEM((rows, depth), BF16),
            pltpu.VMEM((groups, 4 * CHUNK, depth), BF16),
            pltpu.VMEM((depth, kcols), BF16),
            pltpu.VMEM((depth, vcols), BF16),
            pltpu.VMEM((2 * heads, depth), BF16),
            pltpu.VMEM((heads,), F32),
            pltpu.VMEM((depth,), BF16),
            pltpu.VMEM((kcols,), BF16),
            pltpu.VMEM((2, 128), F32),
            pltpu.VMEM((ntp, 2, 128), F32),
            pltpu.VMEM((ntp, *tile), F32),
            pltpu.VMEM((ntp, *tile), F32),
            pltpu.VMEM((2 * ntp, *tile), F32),
            pltpu.VMEM(tile, F32),
            pltpu.VMEM((nx, *tile), F32),
            pltpu.VMEM(tile, F32),
            pltpu.VMEM((nz, *tile), F32),
            pltpu.VMEM(tile, F32),
            pltpu.VMEM((nx, *tile), F32),
            pltpu.VMEM(tile, F32),
            pltpu.VMEM((nz, *tile), F32),
            pltpu.VMEM((2 * hd, vcols), F32),
            pltpu.VMEM(tile, F32),
            dma((8,)),
            dma((2, nchunk)),
            dma((2, groups)),
            dma((nchunk,)),
            dma((groups,)),
            dma((groups,)),
            dma(()),
            dma(()),
            *[dma((ntp - 1,))] * 4,
            *[dma((nx - 1,))] * 2,
            *[dma((nz - 1,))] * 2,
            *[dma((nx - 1,))] * 2,
            *[dma((nz - 1,))] * 2,
            pltpu.SemaphoreType.REGULAR((2,)),
        ],
        compiler_params=pltpu.CompilerParams(
            collective_id=0, has_side_effects=True, vmem_limit_bytes=40 * 1024 * 1024
        ),
        name="prefill",
    )(
        *(
            pltpu.with_memory_space_constraint(operand, pltpu.HBM)
            for operand in (
                prompt_tokens,
                key_weight,
                value_weight,
                input_weight.T,
                forget_weight.T,
                forget_bias,
                new_token,
                new_query,
            )
        )
    )
    results = (key_cache, value_cache, cache_weight, reading)
    key_cache, value_cache, cache_weight, reading = pl.pallas_call(
        put_out,
        out_shape=tuple(jax.ShapeDtypeStruct(r.shape, r.dtype) for r in results),
        in_specs=[vmem] * 4,
        out_specs=[anywhere] * 4,
        scratch_shapes=[dma((4,))],
        compiler_params=pltpu.CompilerParams(vmem_limit_bytes=1024 * 1024),
        name="put_out",
    )(*results)
    return key_cache, value_cache, cache_weight, reading.reshape(-1)


def solution(mesh):
    torus = Mesh(mesh.devices.reshape(8, 4, mesh.shape["tp"]), ("sp_0", "sp_1", "tp"))
    return jax.shard_map(
        body,
        mesh=torus,
        in_specs=(P(SP_TP, None), P(None, "tp"), P(None, "tp"), P(), P(), P(), P(), P("tp")),
        out_specs=(P(SP, "tp"), P(SP, "tp"), P("tp", SP), P("tp")),
        check_vma=False,
    )
```

```python
import functools
import math

import jax
import jax.numpy as jnp
from jax import lax
from jax.experimental import pallas as pl
from jax.experimental.pallas import tpu as pltpu
from jax.sharding import Mesh
from jax.sharding import PartitionSpec as P

DQK = 64
DV = 128
SP = ("sp_0", "sp_1")
SP_TP = ("sp_0", "sp_1", "tp")
MESH = pl.DeviceIdType.MESH
F32 = jnp.float32
BF16 = jnp.bfloat16
CHUNK = 32
EARLY = (2, 4)


def log_sigmoid(v):
    u = jnp.exp(-jnp.abs(v))
    w = 1.0 + u
    grown = w - 1.0
    tail = jnp.where(grown == 0.0, u, jnp.log(w) * (u / jnp.where(grown == 0.0, 1.0, grown)))
    return -(jnp.maximum(-v, 0.0) + tail)


def remote(src, dst, send, recv, where):
    return pltpu.make_async_remote_copy(
        src_ref=src, dst_ref=dst, send_sem=send, recv_sem=recv, device_id=where, device_id_type=MESH
    )


def kernel(
    tok, kw, vw, iw, fw, fb, nt, nq,
    kout, vout, cwout, rdout,
    xown, xsib, gat, wk, wv, wif, bias_v, token_v, query_v,
    tmrow, tmall, lwpay, lwall, wread, cpay, cxs, crow, czs, dpay, dxs, drow, dzs, acc, den,
    wko, query_far, lwsib, ypay, yfar,
    lsem, own_s, own_r, fwd_s, sib_s, sib_r, osib_s, osib_r,
    tm_s, tm_r, lw_s, lw_r, cx_s, cx_r, cz_s, cz_r, dx_s, dx_r, dz_s, dz_r, near_z,
    over_s, over_r, a1_s, a1_r, a2_s, a2_r, b1_s, b1_r, b2_s, b2_r,
    q_s, q_r, lwsib_s, lwsib_r, y_s, y_r,
):
    nz, nx, ntp = (lax.axis_size(a) for a in ("sp_0", "sp_1", "tp"))
    z, x, t = (lax.axis_index(a) for a in ("sp_0", "sp_1", "tp"))
    flip = 1 - 2 * (t % 2)
    sib = t + flip
    up, dn = (t + 2) % ntp, (t + ntp - 2) % ntp
    rows, depth = xown.shape
    nchunk = rows // CHUNK
    groups = gat.shape[0]
    heads = iw.shape[0]
    hd = heads // ntp
    over_lanes = (((1,), (1,)), ((), ()))

    loads = [
        pltpu.make_async_copy(src, dst, lsem.at[i])
        for i, (src, dst) in enumerate(
            (
                (tok, xown),
                (iw, wif.at[pl.ds(0, heads)]),
                (fw, wif.at[pl.ds(heads, heads)]),
                (fb, bias_v),
                (nt, token_v),
                (nq, query_v),
                (kw, wk),
                (vw, wv),
            )
        )
    ]
    for load in loads:
        load.start()

    barrier = pltpu.get_barrier_semaphore()

    def signal(semaphore, axis, to):
        pl.semaphore_signal(semaphore, inc=1, device_id={axis: to}, device_id_type=MESH)

    for d in range(1, ntp):
        signal(barrier, "tp", (t + d) % ntp)
    for d in range(1, nx):
        signal(barrier, "sp_1", (x + d) % nx)
    for d in (1, nz - 1):
        signal(barrier, "sp_0", (z + d) % nz)
    pl.semaphore_wait(barrier, ntp + nx)
    for d in (1, nz - 1):
        signal(near_z.at[0], "sp_0", (z + d) % nz)

    far_t = (t + ntp // 2) % ntp
    slice_rows = wko.shape[3]
    slot = z * nx + x
    over_copies = [
        remote(
            kw.at[pl.ds(pl.multiple_of((2 * slot + i) * slice_rows, slice_rows), slice_rows)],
            wko.at[z, x, i],
            over_s.at[i],
            over_r.at[i],
            {"tp": far_t},
        )
        for i in (0, 1)
    ]
    for copy in over_copies:
        copy.start()

    def own_copies(c):
        piece = xown.at[pl.ds(c * CHUNK, CHUNK)]
        return (
            remote(piece, gat.at[c, pl.ds(0, CHUNK)], own_s.at[0, c], own_r.at[0, c], {"tp": up}),
            remote(
                piece, gat.at[c, pl.ds(CHUNK, CHUNK)], own_s.at[1, c], own_r.at[1, c], {"tp": dn}
            ),
        )

    def send_own(c, carry):
        for copy in own_copies(c):
            copy.start()
        return carry

    def across(src, dst_slots, here, size, axis, send, recv):
        copies = []
        for d in range(1, size):
            to = (here + d) % size
            copies.append(
                remote(src(to), dst_slots.at[here], send.at[d - 1], recv.at[d - 1], {axis: to})
            )
        for copy in copies:
            copy.start()
        return copies

    loads[0].wait()
    lax.fori_loop(0, EARLY[0], send_own, 0)
    own_to_sib = remote(xown, xsib, osib_s, osib_r, {"tp": sib})
    own_to_sib.start()

    pl.semaphore_wait(near_z.at[0], 2)
    for d in (2, nz - 2):
        signal(near_z.at[1], "sp_0", (z + d) % nz)

    for load in loads[1:6]:
        load.wait()
    bias = bias_v[...].reshape(1, heads).T
    gates = lax.dot_general(wif[...], xown[...], over_lanes, preferred_element_type=F32)
    gate_t = gates[0:heads]
    forget_t = log_sigmoid(gates[heads:] + bias)
    later_mask = (
        lax.broadcasted_iota(jnp.int32, (rows, rows), 0)
        > lax.broadcasted_iota(jnp.int32, (rows, rows), 1)
    ).astype(F32).astype(BF16)
    high = forget_t.astype(BF16)
    rest = forget_t - high.astype(F32)
    mid = rest.astype(BF16)
    low = (rest - mid.astype(F32)).astype(BF16)
    suffix = (
        jnp.dot(low, later_mask, preferred_element_type=F32)
        + jnp.dot(mid, later_mask, preferred_element_type=F32)
        + jnp.dot(high, later_mask, preferred_element_type=F32)
    )
    logw = gate_t + suffix
    total = suffix[:, 0:1] + forget_t[:, 0:1]
    top = jnp.max(logw, axis=1, keepdims=True)
    lane = lax.broadcasted_iota(jnp.int32, (heads, 128), 1)
    pairs = jnp.concatenate(
        [jnp.where(lane < 64, total, top), jnp.zeros((128 - heads, 128), F32)], axis=0
    ).T
    tmrow[0:1, :] = pairs[0:1]
    tmrow[1:2, :] = pairs[64:65]
    tm_copies = across(lambda to: tmrow, tmall, t, ntp, "tp", tm_s, tm_r)
    tmall[t] = tmrow[...]

    q_copy = remote(query_v, query_far, q_s, q_r, {"tp": far_t})
    q_copy.start()
    lax.fori_loop(EARLY[0], EARLY[1], send_own, 0)
    pl.semaphore_wait(near_z.at[1], 2)
    for copy in over_copies:
        copy.wait_recv()

    def spread(src, dst, size, axis, here, send, recv):
        copies = [
            remote(src, dst, send.at[d - 1], recv.at[d - 1], {axis: (here + d) % size})
            for d in range(1, size)
        ]
        for copy in copies:
            copy.start()
        return copies

    a_first = spread(wko.at[z, x, 0], wko.at[z, x, 0], nz, "sp_0", z, a1_s, a1_r)
    b_first = spread(wko.at[z, x, 1], wko.at[z, x, 1], nx, "sp_1", x, b1_s, b1_r)

    def project(lhs):
        k = jnp.dot(lhs, wk[...], preferred_element_type=F32).astype(BF16)
        v = jnp.dot(lhs, wv[...], preferred_element_type=F32).astype(BF16)
        return k, v

    def whole_block(src, source):
        k, v = project(src[...])
        at = pl.ds(pl.multiple_of(source * rows, rows), rows)
        kout[at, :] = k
        vout[at, :] = v

    loads[6].wait()
    loads[7].wait()
    whole_block(xown, t)

    for copy in tm_copies:
        copy.wait_recv()
    block_total = jnp.zeros((1, 128), F32)
    mine = block_total
    block_top = None
    for s in reversed(range(ntp)):
        candidate = tmall[s, 1:2, :] + block_total
        block_top = candidate if block_top is None else jnp.maximum(block_top, candidate)
        mine = mine + jnp.where(s > t, tmall[s, 0:1, :], 0.0)
        block_total = block_total + tmall[s, 0:1, :]
    logw = logw + mine.T[0:heads]

    def twice(a):
        return jnp.concatenate(
            [a[j * hd : (j + 1) * hd] for j in range(ntp) for _ in (0, 1)], axis=0
        )

    def is_first(width):
        return lax.broadcasted_iota(jnp.int32, (2 * heads, width), 0) % (2 * hd) < hd

    logw2 = twice(logw)
    packed = jnp.where(is_first(128), logw2[:, :128], logw2[:, 128:])
    for j in range(ntp):
        lwpay[j] = packed[j * 2 * hd : (j + 1) * 2 * hd]
    lw_copies = across(lambda to: lwpay.at[to], lwall, t, ntp, "tp", lw_s, lw_r)
    lwall[t] = lwpay[t]
    lwsib_copy = remote(lwpay.at[(sib + ntp // 2) % ntp], lwsib, lwsib_s, lwsib_r, {"tp": sib})
    lwsib_copy.start()

    lax.fori_loop(EARLY[1], nchunk, send_own, 0)

    token16 = jnp.broadcast_to(token_v[...].reshape(1, depth), (16, depth))
    new_k, new_v = project(token16)
    new_gates = lax.dot_general(wif[...], token16, over_lanes, preferred_element_type=F32)[:, 0:1]
    own_lane = lax.broadcasted_iota(jnp.int32, (hd, 128), 1)
    own_row = lax.broadcasted_iota(jnp.int32, (hd, 128), 0)

    def own_heads(row, owner=t):
        picked = own_lane == owner * hd + own_row
        column = jnp.sum(jnp.where(picked, row, 0.0), axis=1, keepdims=True)
        return jnp.broadcast_to(column, (hd, 128))

    own_head_col = (
        lax.broadcasted_iota(jnp.int32, (heads, hd), 0)
        == t * hd + lax.broadcasted_iota(jnp.int32, (heads, hd), 1)
    )

    def own_columns(column):
        row = jnp.sum(jnp.where(own_head_col, column, 0.0), axis=0, keepdims=True)
        return jnp.broadcast_to(row.T, (hd, 128))

    new_gate = own_columns(new_gates[0:heads])
    new_forget = own_columns(log_sigmoid(new_gates[heads:] + bias))

    cpay[0:hd, :] = own_heads(block_total)
    cpay[hd:, :] = own_heads(block_top)
    cx_copies = across(lambda to: cpay, cxs, x, nx, "sp_1", cx_s, cx_r)
    cxs[x] = cpay[...]

    own_to_sib.wait_recv()
    whole_block(xsib, sib)

    def scanned(slots, size, here):
        behind = jnp.zeros((hd, 128), F32)
        mine = behind
        peak = None
        for s in reversed(range(size)):
            level = slots[s, hd:, :] + behind
            peak = level if peak is None else jnp.maximum(peak, level)
            mine = mine + jnp.where(s > here, slots[s, 0:hd, :], 0.0)
            behind = behind + slots[s, 0:hd, :]
        return behind, peak, mine

    for copy in cx_copies:
        copy.wait_recv()
    row_total, row_peak, later_x = scanned(cxs, nx, x)
    crow[0:hd, :] = row_total
    crow[hd:, :] = row_peak
    cz_copies = across(lambda to: crow, czs, z, nz, "sp_0", cz_s, cz_r)
    czs[z] = crow[...]
    for copy in b_first:
        copy.wait_recv()
    b_second = spread(wko.at[z, :, 1], wko.at[z, :, 1], nz, "sp_0", z, b2_s, b2_r)
    for copy in a_first:
        copy.wait_recv()
    a_second = spread(wko.at[:, x, 0], wko.at[:, x, 0], nx, "sp_1", x, a2_s, a2_r)

    def landed(ref, semaphore):
        pltpu.make_async_copy(ref, ref, semaphore).wait()

    def to_sibling(g):
        return remote(
            gat.at[g, pl.ds(0, 2 * CHUNK)],
            gat.at[g, pl.ds(2 * CHUNK, 2 * CHUNK)],
            sib_s.at[g],
            sib_r.at[g],
            {"tp": sib},
        )

    def ship(g):
        landed(gat.at[g, pl.ds(0, CHUNK)], own_r.at[0, g])
        landed(gat.at[g, pl.ds(CHUNK, CHUNK)], own_r.at[1, g])
        to_sibling(g).start()

    def forward(g, side):
        part = pl.ds(side * CHUNK, CHUNK)
        return remote(
            gat.at[g, part],
            gat.at[nchunk + g // 2, part],
            fwd_s.at[g],
            own_r.at[side, nchunk + g // 2],
            {"tp": dn if side else up},
        )

    def pieces(g):
        e = g // nchunk
        c0 = g + e * (g - 2 * nchunk)
        s0 = (t + ntp - 2 - 2 * e) % ntp
        s1 = (t + 2 + 2 * e) % ntp
        return (
            s0 * rows + c0 * CHUNK,
            s1 * rows + (c0 + e) * CHUNK,
            (s0 + flip) * rows + c0 * CHUNK,
            (s1 + flip) * rows + (c0 + e) * CHUNK,
        )

    def place(lhs, starts):
        k, v = project(lhs)
        for i, start in enumerate(starts):
            at = pl.ds(pl.multiple_of(start, CHUNK), CHUNK)
            kout[at, :] = k[i * CHUNK : (i + 1) * CHUNK]
            vout[at, :] = v[i * CHUNK : (i + 1) * CHUNK]

    def from_sibling(g):
        landed(gat.at[g, pl.ds(2 * CHUNK, 2 * CHUNK)], sib_r.at[g])

    def arrive(g):
        from_sibling(g)
        place(gat[g], pieces(g))

    def near(g, carry):
        ship(g)

        @pl.when(g == nchunk - 2)
        def _():
            forward(0, 0).start()
            forward(1, 1).start()

        @pl.when(g > 0)
        def _():
            arrive(g - 1)

        return carry

    lax.fori_loop(0, nchunk, near, 0)

    def heads_of(flat, wrapped):
        query = jnp.broadcast_to(flat[...].reshape(1, -1), (2 * hd, nq.shape[0])).astype(F32)
        lane_head = lax.broadcasted_iota(jnp.int32, query.shape, 1) // DQK
        row_head = lax.broadcasted_iota(jnp.int32, query.shape, 0)
        row_head = row_head % hd if wrapped else row_head
        return jnp.where(lane_head == row_head, query, 0.0)

    for copy in (*a_second, *b_second, q_copy, lwsib_copy):
        copy.wait_recv()
    queries_far = heads_of(query_far, True).astype(BF16)
    far_top = own_heads(block_top, far_t)
    far_weight = wko[...].reshape(depth, kw.shape[1])
    den_far = jnp.zeros((2 * hd, 1), F32)
    pulled = jnp.zeros((2 * hd, depth), F32)
    for source, tile in ((xown, lwpay[far_t]), (xsib, lwsib[...])):
        keys = jnp.dot(source[...], far_weight, preferred_element_type=F32).astype(BF16)
        score = lax.dot_general(
            queries_far, keys, over_lanes, preferred_element_type=F32
        ) * (1.0 / math.sqrt(DQK))
        level = jnp.concatenate(
            [jnp.exp(tile[0:hd] - far_top), jnp.exp(tile[hd:] - far_top)], axis=1
        )
        weighted = jnp.concatenate([level, level], axis=0) * score
        den_far = den_far + jnp.sum(weighted, axis=1, keepdims=True)
        pulled = pulled + jnp.dot(weighted.astype(BF16), source[...], preferred_element_type=F32)
    half = depth // 2
    first8 = lax.broadcasted_iota(jnp.int32, (2 * hd, 1), 0) < hd
    ypay[:, 0:half] = jnp.where(first8, pulled[:, :half], pulled[:, half:]).astype(BF16)
    den_high = den_far.astype(BF16).astype(F32)
    den_pair = jnp.where(first8, den_high, den_far - den_high)
    ypay[:, half:] = jnp.broadcast_to(den_pair, (2 * hd, 128)).astype(BF16)
    y_copy = remote(ypay, yfar, y_s, y_r, {"tp": far_t})
    y_copy.start()

    def forward_rest(i, carry):
        forward(2 * i, 0).start()
        forward(2 * i + 1, 1).start()
        return carry

    lax.fori_loop(1, nchunk // 2, forward_rest, 0)

    for copy in (*cz_copies, *lw_copies):
        copy.wait_recv()
    _, peak, later_z = scanned(czs, nz, z)
    later = later_x + later_z
    later2 = jnp.concatenate([later, later], axis=0)
    peak2 = jnp.concatenate([peak, peak], axis=0)
    stable = jnp.maximum(new_forget + peak, new_gate)
    shift = new_forget - stable
    shift2 = jnp.concatenate([shift, shift], axis=0)
    zero = jnp.zeros((hd, 128), F32)
    for s in range(ntp):
        whole = lwall[s] + later2
        tile = jnp.exp(whole - peak2)
        cwout[:, s * rows : s * rows + 128] = tile[0:hd]
        cwout[:, s * rows + 128 : (s + 1) * rows] = tile[hd:]
        tile = jnp.exp(whole + shift2)
        wread[2 * s] = jnp.concatenate([tile[0:hd], zero], axis=0)
        wread[2 * s + 1] = jnp.concatenate([tile[hd:], zero], axis=0)

    queries = heads_of(query_v, False)
    queries_low = queries.astype(BF16)
    acc[...] = jnp.zeros_like(acc)
    den[...] = jnp.zeros_like(den)

    def read(unit):
        at = pl.ds(pl.multiple_of(unit * 128, 128), 128)
        score = lax.dot_general(
            queries_low, kout[at, :], over_lanes, preferred_element_type=F32
        ) * (1.0 / math.sqrt(DQK))
        weighted = wread[unit] * score
        den[...] += weighted
        acc[...] += jnp.dot(weighted.astype(BF16), vout[at, :], preferred_element_type=F32)

    def read_near(i, carry):
        away = (i // 4) + (i // 8)
        read(4 * ((t // 2 + away) % (ntp // 2)) + i % 4)
        return carry

    arrive(nchunk - 1)
    lax.fori_loop(0, 12, read_near, 0)
    ship(nchunk)
    y_copy.wait_recv()
    got_first = jnp.dot(yfar[:, 0:half], wv[0:half, :], preferred_element_type=F32)
    got_second = jnp.dot(yfar[:, 0:half], wv[half:, :], preferred_element_type=F32)
    got = got_first[0:hd] + got_second[hd:]
    got_den = yfar[:, half:].astype(F32)
    rescale = jnp.exp(own_heads(block_top) + later + shift)

    for h in range(hd):
        dpay[h : h + 1, :] = (
            acc[h : h + 1, h * DV : (h + 1) * DV]
            + rescale[h : h + 1] * got[h : h + 1, h * DV : (h + 1) * DV]
        )
    dpay[hd:, :] = den[0:hd, :] + jnp.where(
        own_lane == 0, rescale * (got_den[0:hd] + got_den[hd:]), 0.0
    )
    dx_copies = across(lambda to: dpay, dxs, x, nx, "sp_1", dx_s, dx_r)
    dxs[x] = dpay[...]
    new_score = jnp.sum(
        queries[0:hd] * new_k[0:1, :].astype(F32), axis=1, keepdims=True
    ) * (1.0 / math.sqrt(DQK))
    own_term = jnp.exp(new_gate - stable) * new_score
    values = jnp.concatenate(
        [new_v[0:1, h * DV : (h + 1) * DV].astype(F32) for h in range(hd)], axis=0
    )

    def far(g, carry):
        ship(g)
        arrive(g - 1)
        return carry

    lax.fori_loop(nchunk + 1, groups - 1, far, 0)
    for copy in dx_copies:
        copy.wait_recv()
    drow[...] = functools.reduce(jnp.add, [dxs[s] for s in range(nx)])
    dz_copies = across(lambda to: drow, dzs, z, nz, "sp_0", dz_s, dz_r)
    dzs[z] = drow[...]
    last = groups - 1
    arrive(last - 1)
    ship(last)
    ends = pieces(last)
    place(gat[last, 0 : 2 * CHUNK], ends[0:2])
    from_sibling(last)
    place(gat[last, 2 * CHUNK :], ends[2:])
    for copy in dz_copies:
        copy.wait_recv()
    summed = functools.reduce(jnp.add, [dzs[s] for s in range(nz)])
    numerator = summed[0:hd] + own_term * values
    denominator = jnp.sum(summed[hd:], axis=1, keepdims=True) + own_term
    rdout[...] = numerator / jnp.maximum(jnp.abs(denominator), 1.0)

    def own_left(c, carry):
        for copy in own_copies(c):
            copy.wait_send()
        return carry

    lax.fori_loop(0, nchunk, own_left, 0)

    def forwards_left(i, carry):
        forward(2 * i, 0).wait_send()
        forward(2 * i + 1, 1).wait_send()
        return carry

    lax.fori_loop(0, nchunk // 2, forwards_left, 0)

    def sibling_left(g, carry):
        to_sibling(g).wait_send()
        return carry

    lax.fori_loop(0, groups, sibling_left, 0)
    own_to_sib.wait_send()
    for copy in (
        *tm_copies, *lw_copies, *cx_copies, *cz_copies, *dx_copies, *dz_copies,
        *over_copies, *a_first, *a_second, *b_first, *b_second, q_copy, lwsib_copy, y_copy,
    ):
        copy.wait_send()


def put_out(*refs):
    sems = refs[8]
    copies = [pltpu.make_async_copy(refs[i], refs[4 + i], sems.at[i]) for i in range(4)]
    for copy in copies:
        copy.start()
    for copy in copies:
        copy.wait()


def body(
    prompt_tokens,
    key_weight,
    value_weight,
    input_weight,
    forget_weight,
    forget_bias,
    new_token,
    new_query,
):
    nz, nx, ntp = (lax.axis_size(a) for a in ("sp_0", "sp_1", "tp"))
    rows, depth = prompt_tokens.shape
    kcols, vcols = key_weight.shape[1], value_weight.shape[1]
    heads = input_weight.shape[1]
    hd = heads // ntp
    assert hd == 4 and ntp == 8 and rows == 256
    nchunk = rows // CHUNK
    groups = nchunk + nchunk // 2
    anywhere = pl.BlockSpec(memory_space=pltpu.HBM)
    vmem = pl.BlockSpec(memory_space=pltpu.VMEM)
    dma = pltpu.SemaphoreType.DMA
    tile = (2 * hd, 128)
    key_cache, value_cache, cache_weight, reading = pl.pallas_call(
        kernel,
        out_shape=(
            jax.ShapeDtypeStruct((rows * ntp, kcols), BF16),
            jax.ShapeDtypeStruct((rows * ntp, vcols), BF16),
            jax.ShapeDtypeStruct((hd, rows * ntp), F32),
            jax.ShapeDtypeStruct((hd, DV), F32),
        ),
        in_specs=[anywhere] * 8,
        out_specs=[vmem] * 4,
        scratch_shapes=[
            pltpu.VMEM((rows, depth), BF16),
            pltpu.VMEM((rows, depth), BF16),
            pltpu.VMEM((groups, 4 * CHUNK, depth), BF16),
            pltpu.VMEM((depth, kcols), BF16),
            pltpu.VMEM((depth, vcols), BF16),
            pltpu.VMEM((2 * heads, depth), BF16),
            pltpu.VMEM((heads,), F32),
            pltpu.VMEM((depth,), BF16),
            pltpu.VMEM((kcols,), BF16),
            pltpu.VMEM((2, 128), F32),
            pltpu.VMEM((ntp, 2, 128), F32),
            pltpu.VMEM((ntp, *tile), F32),
            pltpu.VMEM((ntp, *tile), F32),
            pltpu.VMEM((2 * ntp, *tile), F32),
            pltpu.VMEM(tile, F32),
            pltpu.VMEM((nx, *tile), F32),
            pltpu.VMEM(tile, F32),
            pltpu.VMEM((nz, *tile), F32),
            pltpu.VMEM(tile, F32),
            pltpu.VMEM((nx, *tile), F32),
            pltpu.VMEM(tile, F32),
            pltpu.VMEM((nz, *tile), F32),
            pltpu.VMEM((2 * hd, vcols), F32),
            pltpu.VMEM(tile, F32),
            pltpu.VMEM((nz, nx, 2, depth // (2 * nz * nx), kcols), BF16),
            pltpu.VMEM((kcols,), BF16),
            pltpu.VMEM(tile, F32),
            pltpu.VMEM((2 * hd, depth // 2 + 128), BF16),
            pltpu.VMEM((2 * hd, depth // 2 + 128), BF16),
            dma((8,)),
            dma((2, nchunk)),
            dma((2, groups)),
            dma((nchunk,)),
            dma((groups,)),
            dma((groups,)),
            dma(()),
            dma(()),
            *[dma((ntp - 1,))] * 4,
            *[dma((nx - 1,))] * 2,
            *[dma((nz - 1,))] * 2,
            *[dma((nx - 1,))] * 2,
            *[dma((nz - 1,))] * 2,
            pltpu.SemaphoreType.REGULAR((2,)),
            *[dma((2,))] * 2,
            *[dma((nz - 1,))] * 2,
            *[dma((nx - 1,))] * 2,
            *[dma((nx - 1,))] * 2,
            *[dma((nz - 1,))] * 2,
            *[dma(())] * 6,
        ],
        compiler_params=pltpu.CompilerParams(
            collective_id=0, has_side_effects=True, vmem_limit_bytes=40 * 1024 * 1024
        ),
        name="prefill",
    )(
        *(
            pltpu.with_memory_space_constraint(operand, pltpu.HBM)
            for operand in (
                prompt_tokens,
                key_weight,
                value_weight,
                input_weight.T,
                forget_weight.T,
                forget_bias,
                new_token,
                new_query,
            )
        )
    )
    results = (key_cache, value_cache, cache_weight, reading)
    key_cache, value_cache, cache_weight, reading = pl.pallas_call(
        put_out,
        out_shape=tuple(jax.ShapeDtypeStruct(r.shape, r.dtype) for r in results),
        in_specs=[vmem] * 4,
        out_specs=[anywhere] * 4,
        scratch_shapes=[dma((4,))],
        compiler_params=pltpu.CompilerParams(vmem_limit_bytes=1024 * 1024),
        name="put_out",
    )(*results)
    return key_cache, value_cache, cache_weight, reading.reshape(-1)


def solution(mesh):
    torus = Mesh(mesh.devices.reshape(8, 4, mesh.shape["tp"]), ("sp_0", "sp_1", "tp"))
    return jax.shard_map(
        body,
        mesh=torus,
        in_specs=(P(SP_TP, None), P(None, "tp"), P(None, "tp"), P(), P(), P(), P(), P("tp")),
        out_specs=(P(SP, "tp"), P(SP, "tp"), P("tp", SP), P("tp")),
        check_vma=False,
    )
```

```python
import functools
import math

import jax
import jax.numpy as jnp
from jax import lax
from jax.experimental import pallas as pl
from jax.experimental.pallas import tpu as pltpu
from jax.sharding import Mesh
from jax.sharding import PartitionSpec as P

DQK = 64
DV = 128
SP = ("sp_0", "sp_1")
SP_TP = ("sp_0", "sp_1", "tp")
MESH = pl.DeviceIdType.MESH
F32 = jnp.float32
BF16 = jnp.bfloat16
CHUNK = 32
EARLY = (2, 4)


def log_sigmoid(v):
    u = jnp.exp(-jnp.abs(v))
    w = 1.0 + u
    grown = w - 1.0
    tail = jnp.where(grown == 0.0, u, jnp.log(w) * (u / jnp.where(grown == 0.0, 1.0, grown)))
    return -(jnp.maximum(-v, 0.0) + tail)


def remote(src, dst, send, recv, where):
    return pltpu.make_async_remote_copy(
        src_ref=src, dst_ref=dst, send_sem=send, recv_sem=recv, device_id=where, device_id_type=MESH
    )


def kernel(
    tok, kw, vw, iw, fw, fb, nt, nq,
    kout, vout, cwout, rdout,
    xown, xsib, gat, wk, wv, wif, bias_v, token_v, query_v,
    tmrow, tmall, lwpay, lwall, wread, cpay, cxs, crow, czs, dpay, dxs, drow, dzs, acc, den,
    wko, query_far, lwsib, ypay, yfar,
    lsem, own_s, own_r, fwd_s, sib_s, sib_r, osib_s, osib_r,
    tm_s, tm_r, lw_s, lw_r, cx_s, cx_r, cz_s, cz_r, dx_s, dx_r, dz_s, dz_r, near_z,
    over_s, over_r, a1_s, a1_r, a2_s, a2_r, b1_s, b1_r, b2_s, b2_r,
    q_s, q_r, lwsib_s, lwsib_r, y_s, y_r,
):
    nz, nx, ntp = (lax.axis_size(a) for a in ("sp_0", "sp_1", "tp"))
    z, x, t = (lax.axis_index(a) for a in ("sp_0", "sp_1", "tp"))
    flip = 1 - 2 * (t % 2)
    sib = t + flip
    up, dn = (t + 2) % ntp, (t + ntp - 2) % ntp
    rows, depth = xown.shape
    nchunk = rows // CHUNK
    groups = gat.shape[0]
    heads = iw.shape[0]
    hd = heads // ntp
    over_lanes = (((1,), (1,)), ((), ()))

    loads = [
        pltpu.make_async_copy(src, dst, lsem.at[i])
        for i, (src, dst) in enumerate(
            (
                (tok, xown),
                (iw, wif.at[pl.ds(0, heads)]),
                (fw, wif.at[pl.ds(heads, heads)]),
                (fb, bias_v),
                (nt, token_v),
                (nq, query_v),
                (kw, wk),
                (vw, wv),
            )
        )
    ]
    for load in loads:
        load.start()

    barrier = pltpu.get_barrier_semaphore()

    def signal(semaphore, axis, to):
        pl.semaphore_signal(semaphore, inc=1, device_id={axis: to}, device_id_type=MESH)

    for d in range(1, ntp):
        signal(barrier, "tp", (t + d) % ntp)

    def along(semaphore, axis, here, size, d):
        @pl.when(here >= d)
        def _():
            signal(semaphore, axis, here - d)

        @pl.when(here + d < size)
        def _():
            signal(semaphore, axis, here + d)

        return (here + size - d) // size + 1 - (here + d) // size

    met = along(barrier, "sp_1", x, nx, 1) + along(barrier, "sp_0", z, nz, 1)
    pl.semaphore_wait(barrier, ntp - 1 + met)
    met = along(near_z.at[0], "sp_1", x, nx, 1) + along(near_z.at[0], "sp_0", z, nz, 1)

    far_t = (t + ntp // 2) % ntp
    slice_rows = wko.shape[3]
    slot = z * nx + x
    over_copies = [
        remote(
            kw.at[pl.ds(pl.multiple_of((2 * slot + i) * slice_rows, slice_rows), slice_rows)],
            wko.at[z, x, i],
            over_s.at[i],
            over_r.at[i],
            {"tp": far_t},
        )
        for i in (0, 1)
    ]
    for copy in over_copies:
        copy.start()

    def own_copies(c):
        piece = xown.at[pl.ds(c * CHUNK, CHUNK)]
        return (
            remote(piece, gat.at[c, pl.ds(0, CHUNK)], own_s.at[0, c], own_r.at[0, c], {"tp": up}),
            remote(
                piece, gat.at[c, pl.ds(CHUNK, CHUNK)], own_s.at[1, c], own_r.at[1, c], {"tp": dn}
            ),
        )

    def send_own(c, carry):
        for copy in own_copies(c):
            copy.start()
        return carry

    def across(src, dst_slots, here, size, axis, send, recv):
        copies = []
        for d in range(1, size):
            to = (here + d) % size
            copies.append(
                remote(src(to), dst_slots.at[here], send.at[d - 1], recv.at[d - 1], {axis: to})
            )
        for copy in copies:
            copy.start()
        return copies

    loads[0].wait()
    lax.fori_loop(0, EARLY[0], send_own, 0)
    own_to_sib = remote(xown, xsib, osib_s, osib_r, {"tp": sib})
    own_to_sib.start()

    pl.semaphore_wait(near_z.at[0], met)
    met = along(near_z.at[1], "sp_1", x, nx, 2) + along(near_z.at[1], "sp_0", z, nz, 2)

    for load in loads[1:6]:
        load.wait()
    bias = bias_v[...].reshape(1, heads).T
    gates = lax.dot_general(wif[...], xown[...], over_lanes, preferred_element_type=F32)
    gate_t = gates[0:heads]
    forget_t = log_sigmoid(gates[heads:] + bias)
    later_mask = (
        lax.broadcasted_iota(jnp.int32, (rows, rows), 0)
        > lax.broadcasted_iota(jnp.int32, (rows, rows), 1)
    ).astype(F32).astype(BF16)
    high = forget_t.astype(BF16)
    rest = forget_t - high.astype(F32)
    mid = rest.astype(BF16)
    low = (rest - mid.astype(F32)).astype(BF16)
    suffix = (
        jnp.dot(low, later_mask, preferred_element_type=F32)
        + jnp.dot(mid, later_mask, preferred_element_type=F32)
        + jnp.dot(high, later_mask, preferred_element_type=F32)
    )
    logw = gate_t + suffix
    total = suffix[:, 0:1] + forget_t[:, 0:1]
    top = jnp.max(logw, axis=1, keepdims=True)
    lane = lax.broadcasted_iota(jnp.int32, (heads, 128), 1)
    pairs = jnp.concatenate(
        [jnp.where(lane < 64, total, top), jnp.zeros((128 - heads, 128), F32)], axis=0
    ).T
    tmrow[0:1, :] = pairs[0:1]
    tmrow[1:2, :] = pairs[64:65]
    pl.semaphore_wait(near_z.at[1], met)
    met = along(near_z.at[2], "sp_0", z, nz, 4)
    tm_copies = across(lambda to: tmrow, tmall, t, ntp, "tp", tm_s, tm_r)
    tmall[t] = tmrow[...]

    q_copy = remote(query_v, query_far, q_s, q_r, {"tp": far_t})
    q_copy.start()
    lax.fori_loop(EARLY[0], EARLY[1], send_own, 0)
    pl.semaphore_wait(near_z.at[2], met)
    for copy in over_copies:
        copy.wait_recv()

    def spread(src, dst, size, axis, here, send, recv):
        copies = [
            remote(src, dst, send.at[d - 1], recv.at[d - 1], {axis: (here + d) % size})
            for d in range(1, size)
        ]
        for copy in copies:
            copy.start()
        return copies

    a_first = spread(wko.at[z, x, 0], wko.at[z, x, 0], nz, "sp_0", z, a1_s, a1_r)
    b_first = spread(wko.at[z, x, 1], wko.at[z, x, 1], nx, "sp_1", x, b1_s, b1_r)

    def project(lhs):
        k = jnp.dot(lhs, wk[...], preferred_element_type=F32).astype(BF16)
        v = jnp.dot(lhs, wv[...], preferred_element_type=F32).astype(BF16)
        return k, v

    def whole_block(src, source):
        k, v = project(src[...])
        at = pl.ds(pl.multiple_of(source * rows, rows), rows)
        kout[at, :] = k
        vout[at, :] = v

    loads[6].wait()
    loads[7].wait()
    whole_block(xown, t)

    for copy in tm_copies:
        copy.wait_recv()
    block_total = jnp.zeros((1, 128), F32)
    mine = block_total
    block_top = None
    for s in reversed(range(ntp)):
        candidate = tmall[s, 1:2, :] + block_total
        block_top = candidate if block_top is None else jnp.maximum(block_top, candidate)
        mine = mine + jnp.where(s > t, tmall[s, 0:1, :], 0.0)
        block_total = block_total + tmall[s, 0:1, :]
    logw = logw + mine.T[0:heads]

    def twice(a):
        return jnp.concatenate(
            [a[j * hd : (j + 1) * hd] for j in range(ntp) for _ in (0, 1)], axis=0
        )

    def is_first(width):
        return lax.broadcasted_iota(jnp.int32, (2 * heads, width), 0) % (2 * hd) < hd

    logw2 = twice(logw)
    packed = jnp.where(is_first(128), logw2[:, :128], logw2[:, 128:])
    for j in range(ntp):
        lwpay[j] = packed[j * 2 * hd : (j + 1) * 2 * hd]
    lw_copies = across(lambda to: lwpay.at[to], lwall, t, ntp, "tp", lw_s, lw_r)
    lwall[t] = lwpay[t]
    lwsib_copy = remote(lwpay.at[(sib + ntp // 2) % ntp], lwsib, lwsib_s, lwsib_r, {"tp": sib})
    lwsib_copy.start()

    lax.fori_loop(EARLY[1], nchunk, send_own, 0)

    for copy in b_first:
        copy.wait_recv()
    b_second = spread(wko.at[z, :, 1], wko.at[z, :, 1], nz, "sp_0", z, b2_s, b2_r)

    token16 = jnp.broadcast_to(token_v[...].reshape(1, depth), (16, depth))
    new_k, new_v = project(token16)
    new_gates = lax.dot_general(wif[...], token16, over_lanes, preferred_element_type=F32)[:, 0:1]
    own_lane = lax.broadcasted_iota(jnp.int32, (hd, 128), 1)
    own_row = lax.broadcasted_iota(jnp.int32, (hd, 128), 0)

    def own_heads(row, owner=t):
        picked = own_lane == owner * hd + own_row
        column = jnp.sum(jnp.where(picked, row, 0.0), axis=1, keepdims=True)
        return jnp.broadcast_to(column, (hd, 128))

    own_head_col = (
        lax.broadcasted_iota(jnp.int32, (heads, hd), 0)
        == t * hd + lax.broadcasted_iota(jnp.int32, (heads, hd), 1)
    )

    def own_columns(column):
        row = jnp.sum(jnp.where(own_head_col, column, 0.0), axis=0, keepdims=True)
        return jnp.broadcast_to(row.T, (hd, 128))

    new_gate = own_columns(new_gates[0:heads])
    new_forget = own_columns(log_sigmoid(new_gates[heads:] + bias))

    cpay[0:hd, :] = own_heads(block_total)
    cpay[hd:, :] = own_heads(block_top)
    cx_copies = across(lambda to: cpay, cxs, x, nx, "sp_1", cx_s, cx_r)
    cxs[x] = cpay[...]

    for copy in a_first:
        copy.wait_recv()
    a_second = spread(wko.at[:, x, 0], wko.at[:, x, 0], nx, "sp_1", x, a2_s, a2_r)
    own_to_sib.wait_recv()
    whole_block(xsib, sib)

    def scanned(slots, size, here):
        behind = jnp.zeros((hd, 128), F32)
        mine = behind
        peak = None
        for s in reversed(range(size)):
            level = slots[s, hd:, :] + behind
            peak = level if peak is None else jnp.maximum(peak, level)
            mine = mine + jnp.where(s > here, slots[s, 0:hd, :], 0.0)
            behind = behind + slots[s, 0:hd, :]
        return behind, peak, mine

    for copy in cx_copies:
        copy.wait_recv()
    row_total, row_peak, later_x = scanned(cxs, nx, x)
    crow[0:hd, :] = row_total
    crow[hd:, :] = row_peak
    cz_copies = across(lambda to: crow, czs, z, nz, "sp_0", cz_s, cz_r)
    czs[z] = crow[...]

    def landed(ref, semaphore):
        pltpu.make_async_copy(ref, ref, semaphore).wait()

    def to_sibling(g):
        return remote(
            gat.at[g, pl.ds(0, 2 * CHUNK)],
            gat.at[g, pl.ds(2 * CHUNK, 2 * CHUNK)],
            sib_s.at[g],
            sib_r.at[g],
            {"tp": sib},
        )

    def ship(g):
        landed(gat.at[g, pl.ds(0, CHUNK)], own_r.at[0, g])
        landed(gat.at[g, pl.ds(CHUNK, CHUNK)], own_r.at[1, g])
        to_sibling(g).start()

    def forward(g, side):
        part = pl.ds(side * CHUNK, CHUNK)
        return remote(
            gat.at[g, part],
            gat.at[nchunk + g // 2, part],
            fwd_s.at[g],
            own_r.at[side, nchunk + g // 2],
            {"tp": dn if side else up},
        )

    def pieces(g):
        e = g // nchunk
        c0 = g + e * (g - 2 * nchunk)
        s0 = (t + ntp - 2 - 2 * e) % ntp
        s1 = (t + 2 + 2 * e) % ntp
        return (
            s0 * rows + c0 * CHUNK,
            s1 * rows + (c0 + e) * CHUNK,
            (s0 + flip) * rows + c0 * CHUNK,
            (s1 + flip) * rows + (c0 + e) * CHUNK,
        )

    def place(lhs, starts):
        k, v = project(lhs)
        for i, start in enumerate(starts):
            at = pl.ds(pl.multiple_of(start, CHUNK), CHUNK)
            kout[at, :] = k[i * CHUNK : (i + 1) * CHUNK]
            vout[at, :] = v[i * CHUNK : (i + 1) * CHUNK]

    def from_sibling(g):
        landed(gat.at[g, pl.ds(2 * CHUNK, 2 * CHUNK)], sib_r.at[g])

    def arrive(g):
        from_sibling(g)
        place(gat[g], pieces(g))

    def near(g, carry):
        ship(g)

        @pl.when(g % 2 == 1)
        def _():
            forward(g - 1, 0).start()
            forward(g, 1).start()

        @pl.when(g > 0)
        def _():
            arrive(g - 1)

        return carry

    lax.fori_loop(0, nchunk // 2, near, 0)

    def heads_of(flat, wrapped):
        query = jnp.broadcast_to(flat[...].reshape(1, -1), (2 * hd, nq.shape[0])).astype(F32)
        lane_head = lax.broadcasted_iota(jnp.int32, query.shape, 1) // DQK
        row_head = lax.broadcasted_iota(jnp.int32, query.shape, 0)
        row_head = row_head % hd if wrapped else row_head
        return jnp.where(lane_head == row_head, query, 0.0)

    for copy in lw_copies:
        copy.wait_recv()
    top = own_heads(block_top)
    top2 = jnp.concatenate([top, top], axis=0)
    zero = jnp.zeros((hd, 128), F32)
    for s in range(ntp):
        tile = jnp.exp(lwall[s] - top2)
        wread[2 * s] = jnp.concatenate([tile[0:hd], zero], axis=0)
        wread[2 * s + 1] = jnp.concatenate([tile[hd:], zero], axis=0)
    queries = heads_of(query_v, False)
    queries_low = queries.astype(BF16)
    acc[...] = jnp.zeros_like(acc)
    den[...] = jnp.zeros_like(den)

    def read(unit):
        at = pl.ds(pl.multiple_of(unit * 128, 128), 128)
        score = lax.dot_general(
            queries_low, kout[at, :], over_lanes, preferred_element_type=F32
        ) * (1.0 / math.sqrt(DQK))
        weighted = wread[unit] * score
        den[...] += weighted
        acc[...] += jnp.dot(weighted.astype(BF16), vout[at, :], preferred_element_type=F32)

    def read_chip(i, carry):
        read(4 * (t // 2) + i)
        return carry

    def read_next(i, half):
        away = 1 + 2 * (i // 2)
        read(4 * ((t // 2 + away) % (ntp // 2)) + 2 * (i % 2) + half)
        return half

    lax.fori_loop(0, 4, read_chip, 0)
    lax.fori_loop(nchunk // 2, nchunk // 2 + 2, near, 0)
    lax.fori_loop(0, 4, read_next, 0)
    near(nchunk - 2, 0)
    for copy in (*a_second, *b_second, q_copy, lwsib_copy):
        copy.wait_recv()
    queries_far = heads_of(query_far, True).astype(BF16)
    far_top = own_heads(block_top, far_t)
    far_weight = wko[...].reshape(depth, kw.shape[1])
    den_far = jnp.zeros((2 * hd, 1), F32)
    pulled = jnp.zeros((2 * hd, depth), F32)
    for source, tile in ((xown, lwpay[far_t]), (xsib, lwsib[...])):
        keys = jnp.dot(source[...], far_weight, preferred_element_type=F32).astype(BF16)
        score = lax.dot_general(
            queries_far, keys, over_lanes, preferred_element_type=F32
        ) * (1.0 / math.sqrt(DQK))
        level = jnp.concatenate(
            [jnp.exp(tile[0:hd] - far_top), jnp.exp(tile[hd:] - far_top)], axis=1
        )
        weighted = jnp.concatenate([level, level], axis=0) * score
        den_far = den_far + jnp.sum(weighted, axis=1, keepdims=True)
        pulled = pulled + jnp.dot(weighted.astype(BF16), source[...], preferred_element_type=F32)
    half = depth // 2
    first8 = lax.broadcasted_iota(jnp.int32, (2 * hd, 1), 0) < hd
    ypay[:, 0:half] = jnp.where(first8, pulled[:, :half], pulled[:, half:]).astype(BF16)
    den_high = den_far.astype(BF16).astype(F32)
    den_pair = jnp.where(first8, den_high, den_far - den_high)
    ypay[:, half:] = jnp.broadcast_to(den_pair, (2 * hd, 128)).astype(BF16)
    y_copy = remote(ypay, yfar, y_s, y_r, {"sp_1": (x + 1) % nx, "tp": far_t})
    y_copy.start()

    near(nchunk - 1, 0)

    arrive(nchunk - 1)
    lax.fori_loop(0, 4, read_next, 1)
    for copy in cz_copies:
        copy.wait_recv()
    _, peak, later_z = scanned(czs, nz, z)
    later = later_x + later_z
    stable = jnp.maximum(new_forget + peak, new_gate)
    shift = new_forget - stable
    ship(nchunk)
    y_copy.wait_recv()
    got_first = jnp.dot(yfar[:, 0:half], wv[0:half, :], preferred_element_type=F32)
    got_second = jnp.dot(yfar[:, 0:half], wv[half:, :], preferred_element_type=F32)
    got = got_first[0:hd] + got_second[hd:]
    got_den = yfar[:, half:].astype(F32)
    before = (x + nx - 1) % nx
    _, _, later_before = scanned(cxs, nx, before)
    rescale = jnp.exp(cxs[before, hd:, :] + later_before + later_z + shift)

    rescale_near = jnp.exp(top + later + shift)

    for h in range(hd):
        dpay[h : h + 1, :] = (
            rescale_near[h : h + 1] * acc[h : h + 1, h * DV : (h + 1) * DV]
            + rescale[h : h + 1] * got[h : h + 1, h * DV : (h + 1) * DV]
        )
    dpay[hd:, :] = rescale_near * den[0:hd, :] + jnp.where(
        own_lane == 0, rescale * (got_den[0:hd] + got_den[hd:]), 0.0
    )
    dx_copies = across(lambda to: dpay, dxs, x, nx, "sp_1", dx_s, dx_r)
    dxs[x] = dpay[...]
    drop = later - peak
    drop2 = jnp.concatenate([drop, drop], axis=0)
    for s in range(ntp):
        tile = jnp.exp(lwall[s] + drop2)
        cwout[:, s * rows : s * rows + 128] = tile[0:hd]
        cwout[:, s * rows + 128 : (s + 1) * rows] = tile[hd:]
    new_score = jnp.sum(
        queries[0:hd] * new_k[0:1, :].astype(F32), axis=1, keepdims=True
    ) * (1.0 / math.sqrt(DQK))
    own_term = jnp.exp(new_gate - stable) * new_score
    values = jnp.concatenate(
        [new_v[0:1, h * DV : (h + 1) * DV].astype(F32) for h in range(hd)], axis=0
    )

    def far(g, carry):
        ship(g)
        arrive(g - 1)
        return carry

    far(nchunk + 1, 0)
    for copy in dx_copies:
        copy.wait_recv()
    drow[...] = functools.reduce(jnp.add, [dxs[s] for s in range(nx)])
    dz_copies = across(lambda to: drow, dzs, z, nz, "sp_0", dz_s, dz_r)
    dzs[z] = drow[...]
    lax.fori_loop(nchunk + 2, groups - 1, far, 0)
    last = groups - 1
    arrive(last - 1)
    ship(last)
    ends = pieces(last)
    place(gat[last, 0 : 2 * CHUNK], ends[0:2])
    from_sibling(last)
    place(gat[last, 2 * CHUNK :], ends[2:])
    for copy in dz_copies:
        copy.wait_recv()
    summed = functools.reduce(jnp.add, [dzs[s] for s in range(nz)])
    numerator = summed[0:hd] + own_term * values
    denominator = jnp.sum(summed[hd:], axis=1, keepdims=True) + own_term
    rdout[...] = numerator / jnp.maximum(jnp.abs(denominator), 1.0)

    def own_left(c, carry):
        for copy in own_copies(c):
            copy.wait_send()
        return carry

    lax.fori_loop(0, nchunk, own_left, 0)

    def forwards_left(i, carry):
        forward(2 * i, 0).wait_send()
        forward(2 * i + 1, 1).wait_send()
        return carry

    lax.fori_loop(0, nchunk // 2, forwards_left, 0)

    def sibling_left(g, carry):
        to_sibling(g).wait_send()
        return carry

    lax.fori_loop(0, groups, sibling_left, 0)
    own_to_sib.wait_send()
    for copy in (
        *tm_copies, *lw_copies, *cx_copies, *cz_copies, *dx_copies, *dz_copies,
        *over_copies, *a_first, *a_second, *b_first, *b_second, q_copy, lwsib_copy, y_copy,
    ):
        copy.wait_send()


def put_out(*refs):
    sems = refs[8]
    copies = [pltpu.make_async_copy(refs[i], refs[4 + i], sems.at[i]) for i in range(4)]
    for copy in copies:
        copy.start()
    for copy in copies:
        copy.wait()


def body(
    prompt_tokens,
    key_weight,
    value_weight,
    input_weight,
    forget_weight,
    forget_bias,
    new_token,
    new_query,
):
    nz, nx, ntp = (lax.axis_size(a) for a in ("sp_0", "sp_1", "tp"))
    rows, depth = prompt_tokens.shape
    kcols, vcols = key_weight.shape[1], value_weight.shape[1]
    heads = input_weight.shape[1]
    hd = heads // ntp
    assert hd == 4 and ntp == 8 and rows == 256
    nchunk = rows // CHUNK
    groups = nchunk + nchunk // 2
    anywhere = pl.BlockSpec(memory_space=pltpu.HBM)
    vmem = pl.BlockSpec(memory_space=pltpu.VMEM)
    dma = pltpu.SemaphoreType.DMA
    tile = (2 * hd, 128)
    key_cache, value_cache, cache_weight, reading = pl.pallas_call(
        kernel,
        out_shape=(
            jax.ShapeDtypeStruct((rows * ntp, kcols), BF16),
            jax.ShapeDtypeStruct((rows * ntp, vcols), BF16),
            jax.ShapeDtypeStruct((hd, rows * ntp), F32),
            jax.ShapeDtypeStruct((hd, DV), F32),
        ),
        in_specs=[anywhere] * 8,
        out_specs=[vmem] * 4,
        scratch_shapes=[
            pltpu.VMEM((rows, depth), BF16),
            pltpu.VMEM((rows, depth), BF16),
            pltpu.VMEM((groups, 4 * CHUNK, depth), BF16),
            pltpu.VMEM((depth, kcols), BF16),
            pltpu.VMEM((depth, vcols), BF16),
            pltpu.VMEM((2 * heads, depth), BF16),
            pltpu.VMEM((heads,), F32),
            pltpu.VMEM((depth,), BF16),
            pltpu.VMEM((kcols,), BF16),
            pltpu.VMEM((2, 128), F32),
            pltpu.VMEM((ntp, 2, 128), F32),
            pltpu.VMEM((ntp, *tile), F32),
            pltpu.VMEM((ntp, *tile), F32),
            pltpu.VMEM((2 * ntp, *tile), F32),
            pltpu.VMEM(tile, F32),
            pltpu.VMEM((nx, *tile), F32),
            pltpu.VMEM(tile, F32),
            pltpu.VMEM((nz, *tile), F32),
            pltpu.VMEM(tile, F32),
            pltpu.VMEM((nx, *tile), F32),
            pltpu.VMEM(tile, F32),
            pltpu.VMEM((nz, *tile), F32),
            pltpu.VMEM((2 * hd, vcols), F32),
            pltpu.VMEM(tile, F32),
            pltpu.VMEM((nz, nx, 2, depth // (2 * nz * nx), kcols), BF16),
            pltpu.VMEM((kcols,), BF16),
            pltpu.VMEM(tile, F32),
            pltpu.VMEM((2 * hd, depth // 2 + 128), BF16),
            pltpu.VMEM((2 * hd, depth // 2 + 128), BF16),
            dma((8,)),
            dma((2, nchunk)),
            dma((2, groups)),
            dma((nchunk,)),
            dma((groups,)),
            dma((groups,)),
            dma(()),
            dma(()),
            *[dma((ntp - 1,))] * 4,
            *[dma((nx - 1,))] * 2,
            *[dma((nz - 1,))] * 2,
            *[dma((nx - 1,))] * 2,
            *[dma((nz - 1,))] * 2,
            pltpu.SemaphoreType.REGULAR((3,)),
            *[dma((2,))] * 2,
            *[dma((nz - 1,))] * 2,
            *[dma((nx - 1,))] * 2,
            *[dma((nx - 1,))] * 2,
            *[dma((nz - 1,))] * 2,
            *[dma(())] * 6,
        ],
        compiler_params=pltpu.CompilerParams(
            collective_id=0, has_side_effects=True, vmem_limit_bytes=40 * 1024 * 1024
        ),
        name="prefill",
    )(
        *(
            pltpu.with_memory_space_constraint(operand, pltpu.HBM)
            for operand in (
                prompt_tokens,
                key_weight,
                value_weight,
                input_weight.T,
                forget_weight.T,
                forget_bias,
                new_token,
                new_query,
            )
        )
    )
    results = (key_cache, value_cache, cache_weight, reading)
    key_cache, value_cache, cache_weight, reading = pl.pallas_call(
        put_out,
        out_shape=tuple(jax.ShapeDtypeStruct(r.shape, r.dtype) for r in results),
        in_specs=[vmem] * 4,
        out_specs=[anywhere] * 4,
        scratch_shapes=[dma((4,))],
        compiler_params=pltpu.CompilerParams(vmem_limit_bytes=1024 * 1024),
        name="put_out",
    )(*results)
    return key_cache, value_cache, cache_weight, reading.reshape(-1)


def solution(mesh):
    torus = Mesh(mesh.devices.reshape(8, 4, mesh.shape["tp"]), ("sp_0", "sp_1", "tp"))
    return jax.shard_map(
        body,
        mesh=torus,
        in_specs=(P(SP_TP, None), P(None, "tp"), P(None, "tp"), P(), P(), P(), P(), P("tp")),
        out_specs=(P(SP, "tp"), P(SP, "tp"), P("tp", SP), P("tp")),
        check_vma=False,
    )
```

```python
import functools
import math

import jax
import jax.numpy as jnp
from jax import lax
from jax.experimental import pallas as pl
from jax.experimental.pallas import tpu as pltpu
from jax.sharding import Mesh
from jax.sharding import PartitionSpec as P

DQK = 64
DV = 128
SP = ("sp_0", "sp_1")
SP_TP = ("sp_0", "sp_1", "tp")
MESH = pl.DeviceIdType.MESH
F32 = jnp.float32
BF16 = jnp.bfloat16
CHUNK = 32
EARLY = (1, 4)


def log_sigmoid(v):
    u = jnp.exp(-jnp.abs(v))
    w = 1.0 + u
    grown = w - 1.0
    tail = jnp.where(grown == 0.0, u, jnp.log(w) * (u / jnp.where(grown == 0.0, 1.0, grown)))
    return -(jnp.maximum(-v, 0.0) + tail)


def remote(src, dst, send, recv, where):
    return pltpu.make_async_remote_copy(
        src_ref=src, dst_ref=dst, send_sem=send, recv_sem=recv, device_id=where, device_id_type=MESH
    )


def kernel(
    tok, kw, vw, iw, fw, fb, nt, nq,
    kout, vout, cwout, rdout,
    xown, xsib, gat, wk, wv, wif, bias_v, token_v, query_v,
    tmrow, tmall, lwpay, lwall, wread, cpay, cxs, crow, czs, dpay, dxs, drow, dzs, acc, den,
    wko, query_far, lwsib, ypay, yfar,
    lsem, own_s, own_r, fwd_s, sib_s, sib_r, osib_s, osib_r,
    tm_s, tm_r, lw_s, lw_r, cx_s, cx_r, cz_s, cz_r, dx_s, dx_r, dz_s, dz_r, near_z,
    over_s, over_r, a1_s, a1_r, a2_s, a2_r, b1_s, b1_r, b2_s, b2_r,
    q_s, q_r, lwsib_s, lwsib_r, y_s, y_r,
):
    nz, nx, ntp = (lax.axis_size(a) for a in ("sp_0", "sp_1", "tp"))
    z, x, t = (lax.axis_index(a) for a in ("sp_0", "sp_1", "tp"))
    flip = 1 - 2 * (t % 2)
    sib = t + flip
    up, dn = (t + 2) % ntp, (t + ntp - 2) % ntp
    rows, depth = xown.shape
    nchunk = rows // CHUNK
    groups = gat.shape[0]
    heads = iw.shape[0]
    hd = heads // ntp
    over_lanes = (((1,), (1,)), ((), ()))

    loads = [
        pltpu.make_async_copy(src, dst, lsem.at[i])
        for i, (src, dst) in enumerate(
            (
                (tok, xown),
                (iw, wif.at[pl.ds(0, heads)]),
                (fw, wif.at[pl.ds(heads, heads)]),
                (fb, bias_v),
                (nt, token_v),
                (nq, query_v),
                (kw, wk),
                (vw, wv),
            )
        )
    ]
    for load in loads:
        load.start()

    barrier = pltpu.get_barrier_semaphore()

    def signal(semaphore, axis, to):
        pl.semaphore_signal(semaphore, inc=1, device_id={axis: to}, device_id_type=MESH)

    for d in range(1, ntp):
        signal(barrier, "tp", (t + d) % ntp)

    def along(semaphore, axis, here, size, d):
        @pl.when(here >= d)
        def _():
            signal(semaphore, axis, here - d)

        @pl.when(here + d < size)
        def _():
            signal(semaphore, axis, here + d)

        return (here + size - d) // size + 1 - (here + d) // size

    met = along(barrier, "sp_1", x, nx, 1) + along(barrier, "sp_0", z, nz, 1)
    pl.semaphore_wait(barrier, ntp - 1 + met)
    met = along(near_z.at[0], "sp_1", x, nx, 1) + along(near_z.at[0], "sp_0", z, nz, 1)

    far_t = (t + ntp // 2) % ntp
    slice_rows = wko.shape[3]
    slot = z * nx + x
    over_copies = [
        remote(
            kw.at[pl.ds(pl.multiple_of((2 * slot + i) * slice_rows, slice_rows), slice_rows)],
            wko.at[z, x, i],
            over_s.at[i],
            over_r.at[i],
            {"tp": far_t},
        )
        for i in (0, 1)
    ]
    for copy in over_copies:
        copy.start()

    def own_copies(c):
        piece = xown.at[pl.ds(c * CHUNK, CHUNK)]
        return (
            remote(piece, gat.at[c, pl.ds(0, CHUNK)], own_s.at[0, c], own_r.at[0, c], {"tp": up}),
            remote(
                piece, gat.at[c, pl.ds(CHUNK, CHUNK)], own_s.at[1, c], own_r.at[1, c], {"tp": dn}
            ),
        )

    def send_own(c, carry):
        for copy in own_copies(c):
            copy.start()
        return carry

    def across(src, dst_slots, here, size, axis, send, recv):
        copies = []
        for d in range(1, size):
            to = (here + d) % size
            copies.append(
                remote(src(to), dst_slots.at[here], send.at[d - 1], recv.at[d - 1], {axis: to})
            )
        for copy in copies:
            copy.start()
        return copies

    loads[0].wait()
    lax.fori_loop(0, EARLY[0], send_own, 0)
    own_to_sib = remote(xown, xsib, osib_s, osib_r, {"tp": sib})
    own_to_sib.start()

    pl.semaphore_wait(near_z.at[0], met)
    met = along(near_z.at[1], "sp_1", x, nx, 2) + along(near_z.at[1], "sp_0", z, nz, 2)

    for load in loads[1:6]:
        load.wait()
    bias = bias_v[...].reshape(1, heads).T
    gates = lax.dot_general(wif[...], xown[...], over_lanes, preferred_element_type=F32)
    gate_t = gates[0:heads]
    forget_t = log_sigmoid(gates[heads:] + bias)
    later_mask = (
        lax.broadcasted_iota(jnp.int32, (rows, rows), 0)
        > lax.broadcasted_iota(jnp.int32, (rows, rows), 1)
    ).astype(F32).astype(BF16)
    high = forget_t.astype(BF16)
    rest = forget_t - high.astype(F32)
    mid = rest.astype(BF16)
    low = (rest - mid.astype(F32)).astype(BF16)
    suffix = (
        jnp.dot(low, later_mask, preferred_element_type=F32)
        + jnp.dot(mid, later_mask, preferred_element_type=F32)
        + jnp.dot(high, later_mask, preferred_element_type=F32)
    )
    logw = gate_t + suffix
    total = suffix[:, 0:1] + forget_t[:, 0:1]
    top = jnp.max(logw, axis=1, keepdims=True)
    lane = lax.broadcasted_iota(jnp.int32, (heads, 128), 1)
    pairs = jnp.concatenate(
        [jnp.where(lane < 64, total, top), jnp.zeros((128 - heads, 128), F32)], axis=0
    ).T
    tmrow[0:1, :] = pairs[0:1]
    tmrow[1:2, :] = pairs[64:65]
    pl.semaphore_wait(near_z.at[1], met)
    met = along(near_z.at[2], "sp_0", z, nz, 4)
    tm_copies = across(lambda to: tmrow, tmall, t, ntp, "tp", tm_s, tm_r)
    tmall[t] = tmrow[...]

    q_copy = remote(query_v, query_far, q_s, q_r, {"tp": far_t})
    q_copy.start()
    lax.fori_loop(EARLY[0], EARLY[1], send_own, 0)
    pl.semaphore_wait(near_z.at[2], met)
    for copy in over_copies:
        copy.wait_recv()

    def spread(src, dst, size, axis, here, send, recv):
        copies = [
            remote(src, dst, send.at[d - 1], recv.at[d - 1], {axis: (here + d) % size})
            for d in range(1, size)
        ]
        for copy in copies:
            copy.start()
        return copies

    a_first = spread(wko.at[z, x, 0], wko.at[z, x, 0], nz, "sp_0", z, a1_s, a1_r)
    b_first = spread(wko.at[z, x, 1], wko.at[z, x, 1], nx, "sp_1", x, b1_s, b1_r)

    def project(lhs):
        k = jnp.dot(lhs, wk[...], preferred_element_type=F32).astype(BF16)
        v = jnp.dot(lhs, wv[...], preferred_element_type=F32).astype(BF16)
        return k, v

    def whole_block(src, source):
        k, v = project(src[...])
        at = pl.ds(pl.multiple_of(source * rows, rows), rows)
        kout[at, :] = k
        vout[at, :] = v

    loads[6].wait()
    loads[7].wait()
    whole_block(xown, t)

    for copy in tm_copies:
        copy.wait_recv()
    block_total = jnp.zeros((1, 128), F32)
    mine = block_total
    block_top = None
    for s in reversed(range(ntp)):
        candidate = tmall[s, 1:2, :] + block_total
        block_top = candidate if block_top is None else jnp.maximum(block_top, candidate)
        mine = mine + jnp.where(s > t, tmall[s, 0:1, :], 0.0)
        block_total = block_total + tmall[s, 0:1, :]
    logw = logw + mine.T[0:heads]

    def twice(a):
        return jnp.concatenate(
            [a[j * hd : (j + 1) * hd] for j in range(ntp) for _ in (0, 1)], axis=0
        )

    def is_first(width):
        return lax.broadcasted_iota(jnp.int32, (2 * heads, width), 0) % (2 * hd) < hd

    logw2 = twice(logw)
    packed = jnp.where(is_first(128), logw2[:, :128], logw2[:, 128:])
    for j in range(ntp):
        lwpay[j] = packed[j * 2 * hd : (j + 1) * 2 * hd]
    lw_copies = across(lambda to: lwpay.at[to], lwall, t, ntp, "tp", lw_s, lw_r)
    lwall[t] = lwpay[t]
    lwsib_copy = remote(lwpay.at[(sib + ntp // 2) % ntp], lwsib, lwsib_s, lwsib_r, {"tp": sib})
    lwsib_copy.start()

    lax.fori_loop(EARLY[1], nchunk, send_own, 0)

    for copy in b_first:
        copy.wait_recv()
    b_second = spread(wko.at[z, :, 1], wko.at[z, :, 1], nz, "sp_0", z, b2_s, b2_r)

    token16 = jnp.broadcast_to(token_v[...].reshape(1, depth), (16, depth))
    new_k, new_v = project(token16)
    new_gates = lax.dot_general(wif[...], token16, over_lanes, preferred_element_type=F32)[:, 0:1]
    own_lane = lax.broadcasted_iota(jnp.int32, (hd, 128), 1)
    own_row = lax.broadcasted_iota(jnp.int32, (hd, 128), 0)

    def own_heads(row, owner=t):
        picked = own_lane == owner * hd + own_row
        column = jnp.sum(jnp.where(picked, row, 0.0), axis=1, keepdims=True)
        return jnp.broadcast_to(column, (hd, 128))

    own_head_col = (
        lax.broadcasted_iota(jnp.int32, (heads, hd), 0)
        == t * hd + lax.broadcasted_iota(jnp.int32, (heads, hd), 1)
    )

    def own_columns(column):
        row = jnp.sum(jnp.where(own_head_col, column, 0.0), axis=0, keepdims=True)
        return jnp.broadcast_to(row.T, (hd, 128))

    new_gate = own_columns(new_gates[0:heads])
    new_forget = own_columns(log_sigmoid(new_gates[heads:] + bias))

    cpay[0:hd, :] = own_heads(block_total)
    cpay[hd:, :] = own_heads(block_top)
    cx_copies = across(lambda to: cpay, cxs, x, nx, "sp_1", cx_s, cx_r)
    cxs[x] = cpay[...]

    for copy in a_first:
        copy.wait_recv()
    a_second = spread(wko.at[:, x, 0], wko.at[:, x, 0], nx, "sp_1", x, a2_s, a2_r)
    own_to_sib.wait_recv()
    whole_block(xsib, sib)

    def scanned(slots, size, here):
        behind = jnp.zeros((hd, 128), F32)
        mine = behind
        peak = None
        for s in reversed(range(size)):
            level = slots[s, hd:, :] + behind
            peak = level if peak is None else jnp.maximum(peak, level)
            mine = mine + jnp.where(s > here, slots[s, 0:hd, :], 0.0)
            behind = behind + slots[s, 0:hd, :]
        return behind, peak, mine

    for copy in cx_copies:
        copy.wait_recv()
    row_total, row_peak, later_x = scanned(cxs, nx, x)
    crow[0:hd, :] = row_total
    crow[hd:, :] = row_peak
    cz_copies = across(lambda to: crow, czs, z, nz, "sp_0", cz_s, cz_r)
    czs[z] = crow[...]

    def landed(ref, semaphore):
        pltpu.make_async_copy(ref, ref, semaphore).wait()

    def to_sibling(g):
        return remote(
            gat.at[g, pl.ds(0, 2 * CHUNK)],
            gat.at[g, pl.ds(2 * CHUNK, 2 * CHUNK)],
            sib_s.at[g],
            sib_r.at[g],
            {"tp": sib},
        )

    def ship(g):
        landed(gat.at[g, pl.ds(0, CHUNK)], own_r.at[0, g])
        landed(gat.at[g, pl.ds(CHUNK, CHUNK)], own_r.at[1, g])
        to_sibling(g).start()

    def forward(g, side):
        part = pl.ds(side * CHUNK, CHUNK)
        return remote(
            gat.at[g, part],
            gat.at[nchunk + g // 2, part],
            fwd_s.at[g],
            own_r.at[side, nchunk + g // 2],
            {"tp": dn if side else up},
        )

    def pieces(g):
        e = g // nchunk
        c0 = g + e * (g - 2 * nchunk)
        s0 = (t + ntp - 2 - 2 * e) % ntp
        s1 = (t + 2 + 2 * e) % ntp
        return (
            s0 * rows + c0 * CHUNK,
            s1 * rows + (c0 + e) * CHUNK,
            (s0 + flip) * rows + c0 * CHUNK,
            (s1 + flip) * rows + (c0 + e) * CHUNK,
        )

    def place(lhs, starts):
        k, v = project(lhs)
        for i, start in enumerate(starts):
            at = pl.ds(pl.multiple_of(start, CHUNK), CHUNK)
            kout[at, :] = k[i * CHUNK : (i + 1) * CHUNK]
            vout[at, :] = v[i * CHUNK : (i + 1) * CHUNK]

    def from_sibling(g):
        landed(gat.at[g, pl.ds(2 * CHUNK, 2 * CHUNK)], sib_r.at[g])

    def arrive(g):
        from_sibling(g)
        place(gat[g], pieces(g))

    def near(g, carry):
        ship(g)

        @pl.when(g % 2 == 1)
        def _():
            forward(g - 1, 0).start()
            forward(g, 1).start()

        @pl.when(g > 0)
        def _():
            arrive(g - 1)

        return carry

    lax.fori_loop(0, nchunk // 2, near, 0)

    def heads_of(flat, wrapped):
        query = jnp.broadcast_to(flat[...].reshape(1, -1), (2 * hd, nq.shape[0])).astype(F32)
        lane_head = lax.broadcasted_iota(jnp.int32, query.shape, 1) // DQK
        row_head = lax.broadcasted_iota(jnp.int32, query.shape, 0)
        row_head = row_head % hd if wrapped else row_head
        return jnp.where(lane_head == row_head, query, 0.0)

    for copy in lw_copies:
        copy.wait_recv()
    top = own_heads(block_top)
    top2 = jnp.concatenate([top, top], axis=0)
    zero = jnp.zeros((hd, 128), F32)
    for s in range(ntp):
        tile = jnp.exp(lwall[s] - top2)
        wread[2 * s] = jnp.concatenate([tile[0:hd], zero], axis=0)
        wread[2 * s + 1] = jnp.concatenate([tile[hd:], zero], axis=0)
    queries = heads_of(query_v, False)
    queries_low = queries.astype(BF16)
    acc[...] = jnp.zeros_like(acc)
    den[...] = jnp.zeros_like(den)

    def read(unit):
        at = pl.ds(pl.multiple_of(unit * 128, 128), 128)
        score = lax.dot_general(
            queries_low, kout[at, :], over_lanes, preferred_element_type=F32
        ) * (1.0 / math.sqrt(DQK))
        weighted = wread[unit] * score
        den[...] += weighted
        acc[...] += jnp.dot(weighted.astype(BF16), vout[at, :], preferred_element_type=F32)

    def read_chip(i, carry):
        read(4 * (t // 2) + i)
        return carry

    def read_next(i, half):
        away = 1 + 2 * (i // 2)
        read(4 * ((t // 2 + away) % (ntp // 2)) + 2 * (i % 2) + half)
        return half

    lax.fori_loop(0, 4, read_chip, 0)
    lax.fori_loop(nchunk // 2, nchunk // 2 + 2, near, 0)
    lax.fori_loop(0, 4, read_next, 0)
    for copy in (*a_second, *b_second, q_copy, lwsib_copy):
        copy.wait_recv()
    queries_far = heads_of(query_far, True).astype(BF16)
    far_top = own_heads(block_top, far_t)
    far_weight = wko[...].reshape(depth, kw.shape[1])
    den_far = jnp.zeros((2 * hd, 1), F32)
    pulled = jnp.zeros((2 * hd, depth), F32)
    for source, tile in ((xown, lwpay[far_t]), (xsib, lwsib[...])):
        keys = jnp.dot(source[...], far_weight, preferred_element_type=F32).astype(BF16)
        score = lax.dot_general(
            queries_far, keys, over_lanes, preferred_element_type=F32
        ) * (1.0 / math.sqrt(DQK))
        level = jnp.concatenate(
            [jnp.exp(tile[0:hd] - far_top), jnp.exp(tile[hd:] - far_top)], axis=1
        )
        weighted = jnp.concatenate([level, level], axis=0) * score
        den_far = den_far + jnp.sum(weighted, axis=1, keepdims=True)
        pulled = pulled + jnp.dot(weighted.astype(BF16), source[...], preferred_element_type=F32)
    half = depth // 2
    first8 = lax.broadcasted_iota(jnp.int32, (2 * hd, 1), 0) < hd
    ypay[:, 0:half] = jnp.where(first8, pulled[:, :half], pulled[:, half:]).astype(BF16)
    den_high = den_far.astype(BF16).astype(F32)
    den_pair = jnp.where(first8, den_high, den_far - den_high)
    ypay[:, half:] = jnp.broadcast_to(den_pair, (2 * hd, 128)).astype(BF16)
    y_copy = remote(ypay, yfar, y_s, y_r, {"sp_1": (x + 1) % nx, "tp": far_t})
    y_copy.start()

    lax.fori_loop(nchunk - 2, nchunk, near, 0)

    arrive(nchunk - 1)
    lax.fori_loop(0, 4, read_next, 1)
    for copy in cz_copies:
        copy.wait_recv()
    _, peak, later_z = scanned(czs, nz, z)
    later = later_x + later_z
    stable = jnp.maximum(new_forget + peak, new_gate)
    shift = new_forget - stable
    ship(nchunk)
    y_copy.wait_recv()
    got_first = jnp.dot(yfar[:, 0:half], wv[0:half, :], preferred_element_type=F32)
    got_second = jnp.dot(yfar[:, 0:half], wv[half:, :], preferred_element_type=F32)
    got = got_first[0:hd] + got_second[hd:]
    got_den = yfar[:, half:].astype(F32)
    before = (x + nx - 1) % nx
    _, _, later_before = scanned(cxs, nx, before)
    rescale = jnp.exp(cxs[before, hd:, :] + later_before + later_z + shift)

    rescale_near = jnp.exp(top + later + shift)

    for h in range(hd):
        dpay[h : h + 1, :] = (
            rescale_near[h : h + 1] * acc[h : h + 1, h * DV : (h + 1) * DV]
            + rescale[h : h + 1] * got[h : h + 1, h * DV : (h + 1) * DV]
        )
    dpay[hd:, :] = rescale_near * den[0:hd, :] + jnp.where(
        own_lane == 0, rescale * (got_den[0:hd] + got_den[hd:]), 0.0
    )
    dx_copies = across(lambda to: dpay, dxs, x, nx, "sp_1", dx_s, dx_r)
    dxs[x] = dpay[...]
    drop = later - peak
    drop2 = jnp.concatenate([drop, drop], axis=0)
    for s in range(ntp):
        tile = jnp.exp(lwall[s] + drop2)
        cwout[:, s * rows : s * rows + 128] = tile[0:hd]
        cwout[:, s * rows + 128 : (s + 1) * rows] = tile[hd:]
    new_score = jnp.sum(
        queries[0:hd] * new_k[0:1, :].astype(F32), axis=1, keepdims=True
    ) * (1.0 / math.sqrt(DQK))
    own_term = jnp.exp(new_gate - stable) * new_score
    values = jnp.concatenate(
        [new_v[0:1, h * DV : (h + 1) * DV].astype(F32) for h in range(hd)], axis=0
    )

    def far(g, carry):
        ship(g)
        arrive(g - 1)
        return carry

    far(nchunk + 1, 0)
    for copy in dx_copies:
        copy.wait_recv()
    drow[...] = functools.reduce(jnp.add, [dxs[s] for s in range(nx)])
    dz_copies = across(lambda to: drow, dzs, z, nz, "sp_0", dz_s, dz_r)
    dzs[z] = drow[...]
    lax.fori_loop(nchunk + 2, groups - 1, far, 0)
    last = groups - 1
    arrive(last - 1)
    ship(last)
    ends = pieces(last)
    place(gat[last, 0 : 2 * CHUNK], ends[0:2])
    from_sibling(last)
    place(gat[last, 2 * CHUNK :], ends[2:])
    for copy in dz_copies:
        copy.wait_recv()
    summed = functools.reduce(jnp.add, [dzs[s] for s in range(nz)])
    numerator = summed[0:hd] + own_term * values
    denominator = jnp.sum(summed[hd:], axis=1, keepdims=True) + own_term
    rdout[...] = numerator / jnp.maximum(jnp.abs(denominator), 1.0)

    def own_left(c, carry):
        for copy in own_copies(c):
            copy.wait_send()
        return carry

    lax.fori_loop(0, nchunk, own_left, 0)

    def forwards_left(i, carry):
        forward(2 * i, 0).wait_send()
        forward(2 * i + 1, 1).wait_send()
        return carry

    lax.fori_loop(0, nchunk // 2, forwards_left, 0)

    def sibling_left(g, carry):
        to_sibling(g).wait_send()
        return carry

    lax.fori_loop(0, groups, sibling_left, 0)
    own_to_sib.wait_send()
    for copy in (
        *tm_copies, *lw_copies, *cx_copies, *cz_copies, *dx_copies, *dz_copies,
        *over_copies, *a_first, *a_second, *b_first, *b_second, q_copy, lwsib_copy, y_copy,
    ):
        copy.wait_send()


def put_out(*refs):
    sems = refs[8]
    copies = [pltpu.make_async_copy(refs[i], refs[4 + i], sems.at[i]) for i in range(4)]
    for copy in copies:
        copy.start()
    for copy in copies:
        copy.wait()


def body(
    prompt_tokens,
    key_weight,
    value_weight,
    input_weight,
    forget_weight,
    forget_bias,
    new_token,
    new_query,
):
    nz, nx, ntp = (lax.axis_size(a) for a in ("sp_0", "sp_1", "tp"))
    rows, depth = prompt_tokens.shape
    kcols, vcols = key_weight.shape[1], value_weight.shape[1]
    heads = input_weight.shape[1]
    hd = heads // ntp
    assert hd == 4 and ntp == 8 and rows == 256
    nchunk = rows // CHUNK
    groups = nchunk + nchunk // 2
    anywhere = pl.BlockSpec(memory_space=pltpu.HBM)
    vmem = pl.BlockSpec(memory_space=pltpu.VMEM)
    dma = pltpu.SemaphoreType.DMA
    tile = (2 * hd, 128)
    key_cache, value_cache, cache_weight, reading = pl.pallas_call(
        kernel,
        out_shape=(
            jax.ShapeDtypeStruct((rows * ntp, kcols), BF16),
            jax.ShapeDtypeStruct((rows * ntp, vcols), BF16),
            jax.ShapeDtypeStruct((hd, rows * ntp), F32),
            jax.ShapeDtypeStruct((hd, DV), F32),
        ),
        in_specs=[anywhere] * 8,
        out_specs=[vmem] * 4,
        scratch_shapes=[
            pltpu.VMEM((rows, depth), BF16),
            pltpu.VMEM((rows, depth), BF16),
            pltpu.VMEM((groups, 4 * CHUNK, depth), BF16),
            pltpu.VMEM((depth, kcols), BF16),
            pltpu.VMEM((depth, vcols), BF16),
            pltpu.VMEM((2 * heads, depth), BF16),
            pltpu.VMEM((heads,), F32),
            pltpu.VMEM((depth,), BF16),
            pltpu.VMEM((kcols,), BF16),
            pltpu.VMEM((2, 128), F32),
            pltpu.VMEM((ntp, 2, 128), F32),
            pltpu.VMEM((ntp, *tile), F32),
            pltpu.VMEM((ntp, *tile), F32),
            pltpu.VMEM((2 * ntp, *tile), F32),
            pltpu.VMEM(tile, F32),
            pltpu.VMEM((nx, *tile), F32),
            pltpu.VMEM(tile, F32),
            pltpu.VMEM((nz, *tile), F32),
            pltpu.VMEM(tile, F32),
            pltpu.VMEM((nx, *tile), F32),
            pltpu.VMEM(tile, F32),
            pltpu.VMEM((nz, *tile), F32),
            pltpu.VMEM((2 * hd, vcols), F32),
            pltpu.VMEM(tile, F32),
            pltpu.VMEM((nz, nx, 2, depth // (2 * nz * nx), kcols), BF16),
            pltpu.VMEM((kcols,), BF16),
            pltpu.VMEM(tile, F32),
            pltpu.VMEM((2 * hd, depth // 2 + 128), BF16),
            pltpu.VMEM((2 * hd, depth // 2 + 128), BF16),
            dma((8,)),
            dma((2, nchunk)),
            dma((2, groups)),
            dma((nchunk,)),
            dma((groups,)),
            dma((groups,)),
            dma(()),
            dma(()),
            *[dma((ntp - 1,))] * 4,
            *[dma((nx - 1,))] * 2,
            *[dma((nz - 1,))] * 2,
            *[dma((nx - 1,))] * 2,
            *[dma((nz - 1,))] * 2,
            pltpu.SemaphoreType.REGULAR((3,)),
            *[dma((2,))] * 2,
            *[dma((nz - 1,))] * 2,
            *[dma((nx - 1,))] * 2,
            *[dma((nx - 1,))] * 2,
            *[dma((nz - 1,))] * 2,
            *[dma(())] * 6,
        ],
        compiler_params=pltpu.CompilerParams(
            collective_id=0, has_side_effects=True, vmem_limit_bytes=40 * 1024 * 1024
        ),
        name="prefill",
    )(
        *(
            pltpu.with_memory_space_constraint(operand, pltpu.HBM)
            for operand in (
                prompt_tokens,
                key_weight,
                value_weight,
                input_weight.T,
                forget_weight.T,
                forget_bias,
                new_token,
                new_query,
            )
        )
    )
    results = (key_cache, value_cache, cache_weight, reading)
    key_cache, value_cache, cache_weight, reading = pl.pallas_call(
        put_out,
        out_shape=tuple(jax.ShapeDtypeStruct(r.shape, r.dtype) for r in results),
        in_specs=[vmem] * 4,
        out_specs=[anywhere] * 4,
        scratch_shapes=[dma((4,))],
        compiler_params=pltpu.CompilerParams(vmem_limit_bytes=1024 * 1024),
        name="put_out",
    )(*results)
    return key_cache, value_cache, cache_weight, reading.reshape(-1)


def solution(mesh):
    torus = Mesh(mesh.devices.reshape(8, 4, mesh.shape["tp"]), ("sp_0", "sp_1", "tp"))
    return jax.shard_map(
        body,
        mesh=torus,
        in_specs=(P(SP_TP, None), P(None, "tp"), P(None, "tp"), P(), P(), P(), P(), P("tp")),
        out_specs=(P(SP, "tp"), P(SP, "tp"), P("tp", SP), P("tp")),
        check_vma=False,
    )
```

```python
import functools
import math

import jax
import jax.numpy as jnp
from jax import lax
from jax.experimental import pallas as pl
from jax.experimental.pallas import tpu as pltpu
from jax.sharding import Mesh
from jax.sharding import PartitionSpec as P

DQK = 64
DV = 128
SP = ("sp_0", "sp_1")
SP_TP = ("sp_0", "sp_1", "tp")
MESH = pl.DeviceIdType.MESH
F32 = jnp.float32
BF16 = jnp.bfloat16
CHUNK = 32
EARLY = (1, 4)


def log_sigmoid(v):
    u = jnp.exp(-jnp.abs(v))
    w = 1.0 + u
    grown = w - 1.0
    tail = jnp.where(grown == 0.0, u, jnp.log(w) * (u / jnp.where(grown == 0.0, 1.0, grown)))
    return -(jnp.maximum(-v, 0.0) + tail)


def remote(src, dst, send, recv, where):
    return pltpu.make_async_remote_copy(
        src_ref=src, dst_ref=dst, send_sem=send, recv_sem=recv, device_id=where, device_id_type=MESH
    )


def kernel(
    tok, kw, vw, iw, fw, fb, nt, nq,
    kout, vout, cwout, rdout,
    xown, xsib, gat, wk, wv, wif, bias_v, token_v, query_v,
    tmrow, tmall, lwpay, lwall, wread, cpay, cxs, crow, czs, dpay, dxs, drow, dzs, acc, den,
    wko, query_far, lwsib, ypay, yfar,
    lsem, own_s, own_r, fwd_s, sib_s, sib_r, osib_s, osib_r,
    tm_s, tm_r, lw_s, lw_r, cx_s, cx_r, cz_s, cz_r, dx_s, dx_r, dz_s, dz_r, near_z,
    over_s, over_r, a1_s, a1_r, a2_s, a2_r, b1_s, b1_r, b2_s, b2_r,
    q_s, q_r, lwsib_s, lwsib_r, y_s, y_r,
):
    nz, nx, ntp = (lax.axis_size(a) for a in ("sp_0", "sp_1", "tp"))
    z, x, t = (lax.axis_index(a) for a in ("sp_0", "sp_1", "tp"))
    flip = 1 - 2 * (t % 2)
    sib = t + flip
    up, dn = (t + 2) % ntp, (t + ntp - 2) % ntp
    rows, depth = xown.shape
    nchunk = rows // CHUNK
    groups = gat.shape[0]
    heads = iw.shape[0]
    hd = heads // ntp
    over_lanes = (((1,), (1,)), ((), ()))

    loads = [
        pltpu.make_async_copy(src, dst, lsem.at[i])
        for i, (src, dst) in enumerate(
            (
                (tok, xown),
                (iw, wif.at[pl.ds(0, heads)]),
                (fw, wif.at[pl.ds(heads, heads)]),
                (fb, bias_v),
                (nt, token_v),
                (nq, query_v),
                (kw, wk),
                (vw, wv),
            )
        )
    ]
    for load in loads:
        load.start()

    barrier = pltpu.get_barrier_semaphore()

    def signal(semaphore, axis, to):
        pl.semaphore_signal(semaphore, inc=1, device_id={axis: to}, device_id_type=MESH)

    for d in range(1, ntp):
        signal(barrier, "tp", (t + d) % ntp)

    def along(semaphore, axis, here, size, d):
        @pl.when(here >= d)
        def _():
            signal(semaphore, axis, here - d)

        @pl.when(here + d < size)
        def _():
            signal(semaphore, axis, here + d)

        return (here + size - d) // size + 1 - (here + d) // size

    met = along(barrier, "sp_1", x, nx, 1) + along(barrier, "sp_0", z, nz, 1)
    pl.semaphore_wait(barrier, ntp - 1 + met)
    met = along(near_z.at[0], "sp_1", x, nx, 1) + along(near_z.at[0], "sp_0", z, nz, 1)

    far_t = (t + ntp // 2) % ntp
    slice_rows = wko.shape[3]
    slot = z * nx + x
    over_copies = [
        remote(
            kw.at[pl.ds(pl.multiple_of((2 * slot + i) * slice_rows, slice_rows), slice_rows)],
            wko.at[z, x, i],
            over_s.at[i],
            over_r.at[i],
            {"tp": far_t},
        )
        for i in (0, 1)
    ]
    for copy in over_copies:
        copy.start()

    def own_copies(c):
        piece = xown.at[pl.ds(c * CHUNK, CHUNK)]
        return (
            remote(piece, gat.at[c, pl.ds(0, CHUNK)], own_s.at[0, c], own_r.at[0, c], {"tp": up}),
            remote(
                piece, gat.at[c, pl.ds(CHUNK, CHUNK)], own_s.at[1, c], own_r.at[1, c], {"tp": dn}
            ),
        )

    def send_own(c, carry):
        for copy in own_copies(c):
            copy.start()
        return carry

    def across(src, dst_slots, here, size, axis, send, recv):
        copies = []
        for d in range(1, size):
            to = (here + d) % size
            copies.append(
                remote(src(to), dst_slots.at[here], send.at[d - 1], recv.at[d - 1], {axis: to})
            )
        for copy in copies:
            copy.start()
        return copies

    loads[0].wait()
    lax.fori_loop(0, EARLY[0], send_own, 0)
    own_to_sib = remote(xown, xsib, osib_s, osib_r, {"tp": sib})
    own_to_sib.start()

    pl.semaphore_wait(near_z.at[0], met)
    met = along(near_z.at[1], "sp_1", x, nx, 2) + along(near_z.at[1], "sp_0", z, nz, 2)

    for load in loads[1:6]:
        load.wait()
    bias = bias_v[...].reshape(1, heads).T
    gates = lax.dot_general(wif[...], xown[...], over_lanes, preferred_element_type=F32)
    gate_t = gates[0:heads]
    forget_t = log_sigmoid(gates[heads:] + bias)
    later_mask = (
        lax.broadcasted_iota(jnp.int32, (rows, rows), 0)
        > lax.broadcasted_iota(jnp.int32, (rows, rows), 1)
    ).astype(F32).astype(BF16)
    high = forget_t.astype(BF16)
    rest = forget_t - high.astype(F32)
    mid = rest.astype(BF16)
    low = (rest - mid.astype(F32)).astype(BF16)
    suffix = (
        jnp.dot(low, later_mask, preferred_element_type=F32)
        + jnp.dot(mid, later_mask, preferred_element_type=F32)
        + jnp.dot(high, later_mask, preferred_element_type=F32)
    )
    logw = gate_t + suffix
    total = suffix[:, 0:1] + forget_t[:, 0:1]
    top = jnp.max(logw, axis=1, keepdims=True)
    lane = lax.broadcasted_iota(jnp.int32, (heads, 128), 1)
    pairs = jnp.concatenate(
        [jnp.where(lane < 64, total, top), jnp.zeros((128 - heads, 128), F32)], axis=0
    ).T
    tmrow[0:1, :] = pairs[0:1]
    tmrow[1:2, :] = pairs[64:65]
    pl.semaphore_wait(near_z.at[1], met)
    met = along(near_z.at[2], "sp_0", z, nz, 4)
    tm_copies = across(lambda to: tmrow, tmall, t, ntp, "tp", tm_s, tm_r)
    tmall[t] = tmrow[...]

    q_copy = remote(query_v, query_far, q_s, q_r, {"tp": far_t})
    q_copy.start()
    lax.fori_loop(EARLY[0], EARLY[1], send_own, 0)
    pl.semaphore_wait(near_z.at[2], met)
    for copy in over_copies:
        copy.wait_recv()

    def spread(src, dst, size, axis, here, send, recv):
        copies = [
            remote(src, dst, send.at[d - 1], recv.at[d - 1], {axis: (here + d) % size})
            for d in range(1, size)
        ]
        for copy in copies:
            copy.start()
        return copies

    a_first = spread(wko.at[z, x, 0], wko.at[z, x, 0], nz, "sp_0", z, a1_s, a1_r)
    b_first = spread(wko.at[z, x, 1], wko.at[z, x, 1], nx, "sp_1", x, b1_s, b1_r)

    def project(lhs):
        k = jnp.dot(lhs, wk[...], preferred_element_type=F32).astype(BF16)
        v = jnp.dot(lhs, wv[...], preferred_element_type=F32).astype(BF16)
        return k, v

    def whole_block(src, source):
        k, v = project(src[...])
        at = pl.ds(pl.multiple_of(source * rows, rows), rows)
        kout[at, :] = k
        vout[at, :] = v

    loads[6].wait()
    loads[7].wait()
    whole_block(xown, t)

    for copy in tm_copies:
        copy.wait_recv()
    block_total = jnp.zeros((1, 128), F32)
    mine = block_total
    block_top = None
    for s in reversed(range(ntp)):
        candidate = tmall[s, 1:2, :] + block_total
        block_top = candidate if block_top is None else jnp.maximum(block_top, candidate)
        mine = mine + jnp.where(s > t, tmall[s, 0:1, :], 0.0)
        block_total = block_total + tmall[s, 0:1, :]
    logw = logw + mine.T[0:heads]

    def twice(a):
        return jnp.concatenate(
            [a[j * hd : (j + 1) * hd] for j in range(ntp) for _ in (0, 1)], axis=0
        )

    def is_first(width):
        return lax.broadcasted_iota(jnp.int32, (2 * heads, width), 0) % (2 * hd) < hd

    logw2 = twice(logw)
    packed = jnp.where(is_first(128), logw2[:, :128], logw2[:, 128:])
    for j in range(ntp):
        lwpay[j] = packed[j * 2 * hd : (j + 1) * 2 * hd]
    lw_copies = across(lambda to: lwpay.at[to], lwall, t, ntp, "tp", lw_s, lw_r)
    lwall[t] = lwpay[t]
    lwsib_copy = remote(lwpay.at[(sib + ntp // 2) % ntp], lwsib, lwsib_s, lwsib_r, {"tp": sib})
    lwsib_copy.start()

    lax.fori_loop(EARLY[1], nchunk, send_own, 0)

    for copy in b_first:
        copy.wait_recv()
    b_second = spread(wko.at[z, :, 1], wko.at[z, :, 1], nz, "sp_0", z, b2_s, b2_r)

    token16 = jnp.broadcast_to(token_v[...].reshape(1, depth), (16, depth))
    new_k, new_v = project(token16)
    new_gates = lax.dot_general(wif[...], token16, over_lanes, preferred_element_type=F32)[:, 0:1]
    own_lane = lax.broadcasted_iota(jnp.int32, (hd, 128), 1)
    own_row = lax.broadcasted_iota(jnp.int32, (hd, 128), 0)

    def own_heads(row, owner=t):
        picked = own_lane == owner * hd + own_row
        column = jnp.sum(jnp.where(picked, row, 0.0), axis=1, keepdims=True)
        return jnp.broadcast_to(column, (hd, 128))

    own_head_col = (
        lax.broadcasted_iota(jnp.int32, (heads, hd), 0)
        == t * hd + lax.broadcasted_iota(jnp.int32, (heads, hd), 1)
    )

    def own_columns(column):
        row = jnp.sum(jnp.where(own_head_col, column, 0.0), axis=0, keepdims=True)
        return jnp.broadcast_to(row.T, (hd, 128))

    new_gate = own_columns(new_gates[0:heads])
    new_forget = own_columns(log_sigmoid(new_gates[heads:] + bias))

    cpay[0:hd, :] = own_heads(block_total)
    cpay[hd:, :] = own_heads(block_top)
    cx_copies = across(lambda to: cpay, cxs, x, nx, "sp_1", cx_s, cx_r)
    cxs[x] = cpay[...]

    own_to_sib.wait_recv()
    whole_block(xsib, sib)
    for copy in a_first:
        copy.wait_recv()
    a_second = spread(wko.at[:, x, 0], wko.at[:, x, 0], nx, "sp_1", x, a2_s, a2_r)

    def scanned(slots, size, here):
        behind = jnp.zeros((hd, 128), F32)
        mine = behind
        peak = None
        for s in reversed(range(size)):
            level = slots[s, hd:, :] + behind
            peak = level if peak is None else jnp.maximum(peak, level)
            mine = mine + jnp.where(s > here, slots[s, 0:hd, :], 0.0)
            behind = behind + slots[s, 0:hd, :]
        return behind, peak, mine

    for copy in cx_copies:
        copy.wait_recv()
    row_total, row_peak, later_x = scanned(cxs, nx, x)
    crow[0:hd, :] = row_total
    crow[hd:, :] = row_peak
    cz_copies = across(lambda to: crow, czs, z, nz, "sp_0", cz_s, cz_r)
    czs[z] = crow[...]

    def landed(ref, semaphore):
        pltpu.make_async_copy(ref, ref, semaphore).wait()

    def to_sibling(g):
        return remote(
            gat.at[g, pl.ds(0, 2 * CHUNK)],
            gat.at[g, pl.ds(2 * CHUNK, 2 * CHUNK)],
            sib_s.at[g],
            sib_r.at[g],
            {"tp": sib},
        )

    def ship(g):
        landed(gat.at[g, pl.ds(0, CHUNK)], own_r.at[0, g])
        landed(gat.at[g, pl.ds(CHUNK, CHUNK)], own_r.at[1, g])
        to_sibling(g).start()

    def forward(g, side):
        part = pl.ds(side * CHUNK, CHUNK)
        return remote(
            gat.at[g, part],
            gat.at[nchunk + g // 2, part],
            fwd_s.at[g],
            own_r.at[side, nchunk + g // 2],
            {"tp": dn if side else up},
        )

    def pieces(g):
        e = g // nchunk
        c0 = g + e * (g - 2 * nchunk)
        s0 = (t + ntp - 2 - 2 * e) % ntp
        s1 = (t + 2 + 2 * e) % ntp
        return (
            s0 * rows + c0 * CHUNK,
            s1 * rows + (c0 + e) * CHUNK,
            (s0 + flip) * rows + c0 * CHUNK,
            (s1 + flip) * rows + (c0 + e) * CHUNK,
        )

    def place(lhs, starts):
        k, v = project(lhs)
        for i, start in enumerate(starts):
            at = pl.ds(pl.multiple_of(start, CHUNK), CHUNK)
            kout[at, :] = k[i * CHUNK : (i + 1) * CHUNK]
            vout[at, :] = v[i * CHUNK : (i + 1) * CHUNK]

    def from_sibling(g):
        landed(gat.at[g, pl.ds(2 * CHUNK, 2 * CHUNK)], sib_r.at[g])

    def arrive(g):
        from_sibling(g)
        place(gat[g], pieces(g))

    def near(g, carry):
        ship(g)

        @pl.when(g % 2 == 1)
        def _():
            forward(g - 1, 0).start()
            forward(g, 1).start()

        @pl.when(g > 0)
        def _():
            arrive(g - 1)

        return carry

    lax.fori_loop(0, nchunk // 2, near, 0)

    def heads_of(flat, wrapped):
        query = jnp.broadcast_to(flat[...].reshape(1, -1), (2 * hd, nq.shape[0])).astype(F32)
        lane_head = lax.broadcasted_iota(jnp.int32, query.shape, 1) // DQK
        row_head = lax.broadcasted_iota(jnp.int32, query.shape, 0)
        row_head = row_head % hd if wrapped else row_head
        return jnp.where(lane_head == row_head, query, 0.0)

    for copy in lw_copies:
        copy.wait_recv()
    top = own_heads(block_top)
    top2 = jnp.concatenate([top, top], axis=0)
    zero = jnp.zeros((hd, 128), F32)
    for s in range(ntp):
        tile = jnp.exp(lwall[s] - top2)
        wread[2 * s] = jnp.concatenate([tile[0:hd], zero], axis=0)
        wread[2 * s + 1] = jnp.concatenate([tile[hd:], zero], axis=0)
    queries = heads_of(query_v, False)
    queries_low = queries.astype(BF16)
    acc[...] = jnp.zeros_like(acc)
    den[...] = jnp.zeros_like(den)

    def read(unit):
        at = pl.ds(pl.multiple_of(unit * 128, 128), 128)
        score = lax.dot_general(
            queries_low, kout[at, :], over_lanes, preferred_element_type=F32
        ) * (1.0 / math.sqrt(DQK))
        weighted = wread[unit] * score
        den[...] += weighted
        acc[...] += jnp.dot(weighted.astype(BF16), vout[at, :], preferred_element_type=F32)

    def read_chip(i, carry):
        read(4 * (t // 2) + i)
        return carry

    def read_next(i, half):
        away = 1 + 2 * (i // 2)
        read(4 * ((t // 2 + away) % (ntp // 2)) + 2 * (i % 2) + half)
        return half

    lax.fori_loop(0, 4, read_chip, 0)
    lax.fori_loop(nchunk // 2, nchunk // 2 + 2, near, 0)
    lax.fori_loop(0, 4, read_next, 0)
    for copy in (*a_second, *b_second, q_copy, lwsib_copy):
        copy.wait_recv()
    queries_far = heads_of(query_far, True).astype(BF16)
    far_top = own_heads(block_top, far_t)
    far_weight = wko[...].reshape(depth, kw.shape[1])
    den_far = jnp.zeros((2 * hd, 1), F32)
    pulled = jnp.zeros((2 * hd, depth), F32)
    for source, tile in ((xown, lwpay[far_t]), (xsib, lwsib[...])):
        keys = jnp.dot(source[...], far_weight, preferred_element_type=F32).astype(BF16)
        score = lax.dot_general(
            queries_far, keys, over_lanes, preferred_element_type=F32
        ) * (1.0 / math.sqrt(DQK))
        level = jnp.concatenate(
            [jnp.exp(tile[0:hd] - far_top), jnp.exp(tile[hd:] - far_top)], axis=1
        )
        weighted = jnp.concatenate([level, level], axis=0) * score
        den_far = den_far + jnp.sum(weighted, axis=1, keepdims=True)
        pulled = pulled + jnp.dot(weighted.astype(BF16), source[...], preferred_element_type=F32)
    half = depth // 2
    first8 = lax.broadcasted_iota(jnp.int32, (2 * hd, 1), 0) < hd
    ypay[:, 0:half] = jnp.where(first8, pulled[:, :half], pulled[:, half:]).astype(BF16)
    den_high = den_far.astype(BF16).astype(F32)
    den_pair = jnp.where(first8, den_high, den_far - den_high)
    ypay[:, half:] = jnp.broadcast_to(den_pair, (2 * hd, 128)).astype(BF16)
    y_copy = remote(ypay, yfar, y_s, y_r, {"sp_1": (x + 1) % nx, "tp": far_t})
    y_copy.start()

    lax.fori_loop(nchunk - 2, nchunk, near, 0)

    arrive(nchunk - 1)
    lax.fori_loop(0, 4, read_next, 1)
    for copy in cz_copies:
        copy.wait_recv()
    _, peak, later_z = scanned(czs, nz, z)
    later = later_x + later_z
    stable = jnp.maximum(new_forget + peak, new_gate)
    shift = new_forget - stable
    ship(nchunk)
    y_copy.wait_recv()
    got_first = jnp.dot(yfar[:, 0:half], wv[0:half, :], preferred_element_type=F32)
    got_second = jnp.dot(yfar[:, 0:half], wv[half:, :], preferred_element_type=F32)
    got = got_first[0:hd] + got_second[hd:]
    got_den = yfar[:, half:].astype(F32)
    before = (x + nx - 1) % nx
    _, _, later_before = scanned(cxs, nx, before)
    rescale = jnp.exp(cxs[before, hd:, :] + later_before + later_z + shift)

    rescale_near = jnp.exp(top + later + shift)

    for h in range(hd):
        dpay[h : h + 1, :] = (
            rescale_near[h : h + 1] * acc[h : h + 1, h * DV : (h + 1) * DV]
            + rescale[h : h + 1] * got[h : h + 1, h * DV : (h + 1) * DV]
        )
    dpay[hd:, :] = rescale_near * den[0:hd, :] + jnp.where(
        own_lane == 0, rescale * (got_den[0:hd] + got_den[hd:]), 0.0
    )
    dx_copies = across(lambda to: dpay, dxs, x, nx, "sp_1", dx_s, dx_r)
    dxs[x] = dpay[...]
    new_score = jnp.sum(
        queries[0:hd] * new_k[0:1, :].astype(F32), axis=1, keepdims=True
    ) * (1.0 / math.sqrt(DQK))
    own_term = jnp.exp(new_gate - stable) * new_score
    values = jnp.concatenate(
        [new_v[0:1, h * DV : (h + 1) * DV].astype(F32) for h in range(hd)], axis=0
    )

    def far(g, carry):
        ship(g)
        arrive(g - 1)
        return carry

    for copy in dx_copies:
        copy.wait_recv()
    drow[...] = functools.reduce(jnp.add, [dxs[s] for s in range(nx)])
    dz_copies = across(lambda to: drow, dzs, z, nz, "sp_0", dz_s, dz_r)
    dzs[z] = drow[...]
    drop = later - peak
    drop2 = jnp.concatenate([drop, drop], axis=0)
    for s in range(ntp):
        tile = jnp.exp(lwall[s] + drop2)
        cwout[:, s * rows : s * rows + 128] = tile[0:hd]
        cwout[:, s * rows + 128 : (s + 1) * rows] = tile[hd:]
    lax.fori_loop(nchunk + 1, groups - 1, far, 0)
    last = groups - 1
    arrive(last - 1)
    ship(last)
    ends = pieces(last)
    place(gat[last, 0 : 2 * CHUNK], ends[0:2])
    from_sibling(last)
    place(gat[last, 2 * CHUNK :], ends[2:])
    for copy in dz_copies:
        copy.wait_recv()
    summed = functools.reduce(jnp.add, [dzs[s] for s in range(nz)])
    numerator = summed[0:hd] + own_term * values
    denominator = jnp.sum(summed[hd:], axis=1, keepdims=True) + own_term
    rdout[...] = numerator / jnp.maximum(jnp.abs(denominator), 1.0)

    def own_left(c, carry):
        for copy in own_copies(c):
            copy.wait_send()
        return carry

    lax.fori_loop(0, nchunk, own_left, 0)

    def forwards_left(i, carry):
        forward(2 * i, 0).wait_send()
        forward(2 * i + 1, 1).wait_send()
        return carry

    lax.fori_loop(0, nchunk // 2, forwards_left, 0)

    def sibling_left(g, carry):
        to_sibling(g).wait_send()
        return carry

    lax.fori_loop(0, groups, sibling_left, 0)
    own_to_sib.wait_send()
    for copy in (
        *tm_copies, *lw_copies, *cx_copies, *cz_copies, *dx_copies, *dz_copies,
        *over_copies, *a_first, *a_second, *b_first, *b_second, q_copy, lwsib_copy, y_copy,
    ):
        copy.wait_send()


def put_out(*refs):
    sems = refs[8]
    copies = [pltpu.make_async_copy(refs[i], refs[4 + i], sems.at[i]) for i in range(4)]
    for copy in copies:
        copy.start()
    for copy in copies:
        copy.wait()


def body(
    prompt_tokens,
    key_weight,
    value_weight,
    input_weight,
    forget_weight,
    forget_bias,
    new_token,
    new_query,
):
    nz, nx, ntp = (lax.axis_size(a) for a in ("sp_0", "sp_1", "tp"))
    rows, depth = prompt_tokens.shape
    kcols, vcols = key_weight.shape[1], value_weight.shape[1]
    heads = input_weight.shape[1]
    hd = heads // ntp
    assert hd == 4 and ntp == 8 and rows == 256
    nchunk = rows // CHUNK
    groups = nchunk + nchunk // 2
    anywhere = pl.BlockSpec(memory_space=pltpu.HBM)
    vmem = pl.BlockSpec(memory_space=pltpu.VMEM)
    dma = pltpu.SemaphoreType.DMA
    tile = (2 * hd, 128)
    key_cache, value_cache, cache_weight, reading = pl.pallas_call(
        kernel,
        out_shape=(
            jax.ShapeDtypeStruct((rows * ntp, kcols), BF16),
            jax.ShapeDtypeStruct((rows * ntp, vcols), BF16),
            jax.ShapeDtypeStruct((hd, rows * ntp), F32),
            jax.ShapeDtypeStruct((hd, DV), F32),
        ),
        in_specs=[anywhere] * 8,
        out_specs=[vmem] * 4,
        scratch_shapes=[
            pltpu.VMEM((rows, depth), BF16),
            pltpu.VMEM((rows, depth), BF16),
            pltpu.VMEM((groups, 4 * CHUNK, depth), BF16),
            pltpu.VMEM((depth, kcols), BF16),
            pltpu.VMEM((depth, vcols), BF16),
            pltpu.VMEM((2 * heads, depth), BF16),
            pltpu.VMEM((heads,), F32),
            pltpu.VMEM((depth,), BF16),
            pltpu.VMEM((kcols,), BF16),
            pltpu.VMEM((2, 128), F32),
            pltpu.VMEM((ntp, 2, 128), F32),
            pltpu.VMEM((ntp, *tile), F32),
            pltpu.VMEM((ntp, *tile), F32),
            pltpu.VMEM((2 * ntp, *tile), F32),
            pltpu.VMEM(tile, F32),
            pltpu.VMEM((nx, *tile), F32),
            pltpu.VMEM(tile, F32),
            pltpu.VMEM((nz, *tile), F32),
            pltpu.VMEM(tile, F32),
            pltpu.VMEM((nx, *tile), F32),
            pltpu.VMEM(tile, F32),
            pltpu.VMEM((nz, *tile), F32),
            pltpu.VMEM((2 * hd, vcols), F32),
            pltpu.VMEM(tile, F32),
            pltpu.VMEM((nz, nx, 2, depth // (2 * nz * nx), kcols), BF16),
            pltpu.VMEM((kcols,), BF16),
            pltpu.VMEM(tile, F32),
            pltpu.VMEM((2 * hd, depth // 2 + 128), BF16),
            pltpu.VMEM((2 * hd, depth // 2 + 128), BF16),
            dma((8,)),
            dma((2, nchunk)),
            dma((2, groups)),
            dma((nchunk,)),
            dma((groups,)),
            dma((groups,)),
            dma(()),
            dma(()),
            *[dma((ntp - 1,))] * 4,
            *[dma((nx - 1,))] * 2,
            *[dma((nz - 1,))] * 2,
            *[dma((nx - 1,))] * 2,
            *[dma((nz - 1,))] * 2,
            pltpu.SemaphoreType.REGULAR((3,)),
            *[dma((2,))] * 2,
            *[dma((nz - 1,))] * 2,
            *[dma((nx - 1,))] * 2,
            *[dma((nx - 1,))] * 2,
            *[dma((nz - 1,))] * 2,
            *[dma(())] * 6,
        ],
        compiler_params=pltpu.CompilerParams(
            collective_id=0, has_side_effects=True, vmem_limit_bytes=40 * 1024 * 1024
        ),
        name="prefill",
    )(
        *(
            pltpu.with_memory_space_constraint(operand, pltpu.HBM)
            for operand in (
                prompt_tokens,
                key_weight,
                value_weight,
                input_weight.T,
                forget_weight.T,
                forget_bias,
                new_token,
                new_query,
            )
        )
    )
    results = (key_cache, value_cache, cache_weight, reading)
    key_cache, value_cache, cache_weight, reading = pl.pallas_call(
        put_out,
        out_shape=tuple(jax.ShapeDtypeStruct(r.shape, r.dtype) for r in results),
        in_specs=[vmem] * 4,
        out_specs=[anywhere] * 4,
        scratch_shapes=[dma((4,))],
        compiler_params=pltpu.CompilerParams(vmem_limit_bytes=1024 * 1024),
        name="put_out",
    )(*results)
    return key_cache, value_cache, cache_weight, reading.reshape(-1)


def solution(mesh):
    torus = Mesh(mesh.devices.reshape(8, 4, mesh.shape["tp"]), ("sp_0", "sp_1", "tp"))
    return jax.shard_map(
        body,
        mesh=torus,
        in_specs=(P(SP_TP, None), P(None, "tp"), P(None, "tp"), P(), P(), P(), P(), P("tp")),
        out_specs=(P(SP, "tp"), P(SP, "tp"), P("tp", SP), P("tp")),
        check_vma=False,
    )
```
